256 devices in a mesh: ra: 32 (over z, y), cb: 4 (over x), dp: 2 (over core).
Axes of the slice: x: 4, y: 4, z: 8, core: 2. Of those that a mesh axis runs over, the one named last changes fastest.
Arguments:
- stream: bfloat16 [4, 64, 4096], P('dp', None, 'ra'), may hold values from -16 to 16
- norm_gain: bfloat16 [2, 4096], P(None, 'ra'), may hold values from 0.099609375 to 1.8984375
- gate_weight: bfloat16 [2, 4096, 12288], P(None, 'ra', 'cb'), may hold values from -0.09375 to 0.09375
- value_weight: bfloat16 [2, 4096, 12288], P(None, 'ra', 'cb'), may hold values from -0.09375 to 0.09375
- gate_taps: bfloat16 [2, 3, 12288], P(None, None, 'cb'), may hold values from -3 to 3
- value_taps: bfloat16 [2, 3, 12288], P(None, None, 'cb'), may hold values from -3 to 3
- gate_bias: bfloat16 [2, 12288], P(None, 'cb'), may hold values from -3 to 3
- value_bias: bfloat16 [2, 12288], P(None, 'cb'), may hold values from -3 to 3
- down_weight: bfloat16 [2, 12288, 4096], P(None, 'cb', 'ra'), may hold values from -0.0546875 to 0.0546875
- final_gain: bfloat16 [4096], P('ra'), may hold values from 0.099609375 to 1.8984375
Outputs:
- mixed: bfloat16 [4, 64, 4096], P('dp', None, 'ra')
The draws below stay inside these ranges and needn't reach their ends.
All inputs are finite; a program needn't handle non-finite values.
Results may differ from the reference program's by a relative error of at most 0.035.
Values may be sent and summed in bfloat16 or wider, within the bound.
No kernel may reach another device: no remote copies, remote signals or barrier semaphores. Data moves between devices by JAX's collectives and lax.ppermute only.
A program may use at most 64 MiB of HBM per device.

```python
import jax
import jax.numpy as jnp
from jax import lax

D = 4096
FF = 12288
TAPS = 3
LAYERS = 2
LEN = 64
BATCH = 4
N_CB = 4


def draw_stream(key, part):
    first, second, third = jax.random.split(key, 3)
    base = jnp.clip(jax.random.normal(first, (BATCH, LEN, D), jnp.float32), -4.0, 4.0)
    channel = jnp.exp(jax.random.uniform(second, (D // 16,), jnp.float32, -1.1, 1.1))
    rowscale = jnp.exp(jax.random.uniform(third, (BATCH, LEN), jnp.float32, -0.7, 0.7))
    values = base * jnp.repeat(channel, 16)[None, None, :] * rowscale[:, :, None]
    return jnp.clip(values, -16.0, 16.0).astype(jnp.bfloat16)


def steps_of(rng, extent, cuts, smallest, largest):
    def one(position, blocks):
        heights = jax.random.uniform(jax.random.fold_in(jax.random.fold_in(rng, 6), position), (blocks,), jnp.float32, smallest / len(cuts), largest / len(cuts))
        return jnp.repeat(jnp.exp(heights), extent[position] // blocks).reshape((-1,) + (1,) * (len(extent) - position - 1))

    gain = one(*cuts[0])
    for cut in cuts[1:]:
        gain = gain * one(*cut)
    return gain


def bell_draw(stream_key, shape, spread, most, shards=(), kind=jnp.bfloat16):
    values = spread * jax.random.normal(stream_key, shape, jnp.float32)
    if shards:
        values = values * steps_of(stream_key, shape, shards, -0.22, 0.18)
    return jnp.clip(values, -most, most).astype(kind)


def setup_inputs(seed: int = 0) -> dict:
    keys = jax.random.split(jax.random.key(seed), 11)
    stream = draw_stream(jax.random.fold_in(keys[10], 71), 0)
    norm_gain = jnp.clip(1.0 + 0.18 * jax.random.normal(keys[1], (LAYERS, D), jnp.float32), 0.099609375, 1.8984375).astype(jnp.bfloat16)
    gate_weight = bell_draw(keys[2], (LAYERS, D, FF), D ** -0.5, 0.09375, ((1, 32), (2, 4)))
    value_weight = bell_draw(keys[3], (LAYERS, D, FF), D ** -0.5, 0.09375, ((1, 32), (2, 4)))
    gate_taps = bell_draw(keys[4], (LAYERS, TAPS, FF), 0.577, 3.0, ((2, 4),))
    value_taps = bell_draw(keys[5], (LAYERS, TAPS, FF), 0.577, 3.0, ((2, 4),))
    gate_bias = bell_draw(keys[6], (LAYERS, FF), 0.5, 3.0, ((1, 4),))
    value_bias = bell_draw(keys[7], (LAYERS, FF), 0.5, 3.0, ((1, 4),))
    down_weight = bell_draw(keys[8], (LAYERS, FF, D), FF ** -0.5, 0.0546875, ((1, 4), (2, 32)))
    final_gain = jnp.clip(1.0 + 0.18 * jax.random.normal(keys[9], (D,), jnp.float32), 0.099609375, 1.8984375).astype(jnp.bfloat16)
    return dict(stream=stream, norm_gain=norm_gain, gate_weight=gate_weight, value_weight=value_weight, gate_taps=gate_taps, value_taps=value_taps, gate_bias=gate_bias, value_bias=value_bias, down_weight=down_weight, final_gain=final_gain)


EPS = 1e-06

def rms_scaled(stream_in, gain_row):
    values = stream_in.astype(jnp.float32)
    squares = lax.optimization_barrier(jnp.sum(values * values, axis=-1, keepdims=True))
    return values * lax.rsqrt(squares / D + EPS) * gain_row.astype(jnp.float32)

def causal_mix(up_rows, taps, bias):
    length = up_rows.shape[1]
    count = taps.shape[0]
    padded = jnp.pad(up_rows.astype(jnp.float32), ((0, 0), (count - 1, 0), (0, 0)))
    result = jnp.zeros(up_rows.shape, jnp.float32) + bias.astype(jnp.float32)
    for tap_index in range(count):
        result = result + padded[:, tap_index:tap_index + length] * taps[tap_index].astype(jnp.float32)
    return result

def reference(stream, norm_gain, gate_weight, value_weight, gate_taps, value_taps, gate_bias, value_bias, down_weight, final_gain):
    batch_rows, length, width = stream.shape
    current = stream
    ff_block = FF // N_CB
    for layer_index in range(LAYERS):
        normed = rms_scaled(current, norm_gain[layer_index]).astype(jnp.bfloat16).reshape(-1, width)
        gate_up = jnp.dot(normed, gate_weight[layer_index], preferred_element_type=jnp.float32).astype(jnp.bfloat16)
        value_up = jnp.dot(normed, value_weight[layer_index], preferred_element_type=jnp.float32).astype(jnp.bfloat16)
        gate_conv = causal_mix(gate_up.reshape(batch_rows, length, FF), gate_taps[layer_index], gate_bias[layer_index])
        value_conv = causal_mix(value_up.reshape(batch_rows, length, FF), value_taps[layer_index], value_bias[layer_index])
        hidden = (jax.nn.gelu(gate_conv) * value_conv).astype(jnp.bfloat16).reshape(-1, FF)
        branch = jnp.zeros((hidden.shape[0], width), jnp.float32)
        for block_index in range(N_CB):
            lower = block_index * ff_block
            term = jnp.dot(hidden[:, lower:lower + ff_block], down_weight[layer_index, lower:lower + ff_block], preferred_element_type=jnp.float32)
            rounded = lax.optimization_barrier(term.astype(jnp.bfloat16))
            branch = branch + rounded.astype(jnp.float32)
        current = (0.5 * current.astype(jnp.float32) + branch.reshape(batch_rows, length, width)).astype(jnp.bfloat16)
    return rms_scaled(current, final_gain).astype(jnp.bfloat16)
```

```python
import jax
import jax.numpy as jnp
from jax import lax
from jax.sharding import Mesh
from jax.sharding import PartitionSpec as P

D = 4096
LAYERS = 2
RA = ("ra_0", "ra_1")
EPS = 1e-06
F32 = jnp.float32
BF16 = jnp.bfloat16
TN = (((0,), (0,)), ((), ()))


def exchanged(x, axis):
    return lax.all_to_all(x, axis, split_axis=0, concat_axis=0, tiled=True)


def to_everyone(x, axis):
    copies = jnp.broadcast_to(x[None], (lax.axis_size(axis), *x.shape))
    return exchanged(copies, axis)


def two_halves(row):
    high = row.astype(BF16)
    low = (row - high.astype(F32)).astype(BF16)
    return jnp.concatenate([high, low], axis=0)


def shifted(x, by, position):
    moved = jnp.pad(x, ((0, 0), (by, 0)))[:, : x.shape[1]]
    return jnp.where(position >= by, moved, 0.0)


def causal_mix(rows, columns, position):
    x = rows.astype(F32)
    return (
        columns[:, 3:4]
        + shifted(x, 2, position) * columns[:, 0:1]
        + shifted(x, 1, position) * columns[:, 1:2]
        + x * columns[:, 2:3]
    )


def body(
    stream,
    norm_gain,
    gate_weight,
    value_weight,
    gate_taps,
    value_taps,
    gate_bias,
    value_bias,
    down_weight,
    final_gain,
):
    batch_rows, length, width = stream.shape
    tokens = batch_rows * length
    members = lax.axis_size(RA)
    units = gate_weight.shape[2] // members
    position = lax.broadcasted_iota(jnp.int32, (1, tokens), 1) % length
    lower = lax.axis_index(RA) * units
    table = jnp.concatenate(
        [gate_taps, gate_bias[:, None], value_taps, value_bias[:, None]], axis=1
    )
    table = lax.dynamic_slice_in_dim(table, lower, units, 2)
    table = jnp.swapaxes(table, 1, 2).astype(F32)
    gains = norm_gain.astype(F32)[:, :, None]
    current = stream.reshape(tokens, width).T
    for layer in range(LAYERS):
        values = current.astype(F32)
        squares = jnp.sum(values * values, axis=0, keepdims=True)
        gained = (values * gains[layer]).astype(BF16)
        gate = lax.dot_general(gate_weight[layer], gained, TN, preferred_element_type=F32)
        value = lax.dot_general(value_weight[layer], gained, TN, preferred_element_type=F32)
        parts = jnp.concatenate(
            [
                gate.astype(BF16).reshape(members, units, tokens),
                value.astype(BF16).reshape(members, units, tokens),
                jnp.broadcast_to(two_halves(squares)[None], (members, 2, tokens)),
            ],
            axis=1,
        )
        total = exchanged(parts, RA).astype(F32).sum(axis=0)
        scale = lax.rsqrt((total[2 * units] + total[2 * units + 1])[None] / D + EPS)
        gate_up = (total[:units] * scale).astype(BF16)
        value_up = (total[units : 2 * units] * scale).astype(BF16)
        gate_conv = causal_mix(gate_up, table[layer, :, 0:4], position)
        value_conv = causal_mix(value_up, table[layer, :, 4:8], position)
        hidden = (jax.nn.gelu(gate_conv) * value_conv).astype(BF16)
        block = to_everyone(hidden, RA).reshape(-1, tokens)
        term = lax.dot_general(down_weight[layer], block, TN, preferred_element_type=F32)
        branch = to_everyone(term.astype(BF16), "cb").astype(F32).sum(axis=0)
        current = (0.5 * values + branch).astype(BF16)
    values = current.astype(F32)
    squares = jnp.sum(values * values, axis=0, keepdims=True)
    total = to_everyone(two_halves(squares), RA).astype(F32).sum(axis=(0, 1))
    mixed = values * lax.rsqrt(total[None] / D + EPS) * final_gain.astype(F32)[:, None]
    return mixed.astype(BF16).T.reshape(batch_rows, length, width)


def solution(mesh):
    split = Mesh(
        mesh.devices.reshape(8, 4, mesh.shape["cb"], mesh.shape["dp"]), ("ra_0", "ra_1", "cb", "dp")
    )
    return jax.shard_map(
        body,
        mesh=split,
        in_specs=(
            P("dp", None, RA),
            P(None, RA),
            P(None, RA, "cb"),
            P(None, RA, "cb"),
            P(None, None, "cb"),
            P(None, None, "cb"),
            P(None, "cb"),
            P(None, "cb"),
            P(None, "cb", RA),
            P(RA),
        ),
        out_specs=P("dp", None, RA),
        check_vma=False,
    )
```

```python
import jax
import jax.numpy as jnp
from jax import lax
from jax.sharding import Mesh
from jax.sharding import PartitionSpec as P

D = 4096
LAYERS = 2
LANES = 128
EPS = 1e-06
F32 = jnp.float32
BF16 = jnp.bfloat16
TN = (((0,), (0,)), ((), ()))


def exchanged(x, axis):
    return lax.all_to_all(x, axis, split_axis=0, concat_axis=0, tiled=True)


def to_everyone(x, axis):
    copies = jnp.broadcast_to(x[None], (lax.axis_size(axis), *x.shape))
    return exchanged(copies, axis)


def two_halves(row):
    high = row.astype(BF16)
    low = (row - high.astype(F32)).astype(BF16)
    return jnp.concatenate([high, low], axis=0)


def shifted(x, by, position):
    moved = jnp.pad(x, ((0, 0), (by, 0)))[:, : x.shape[1]]
    return jnp.where(position >= by, moved, 0.0)


def causal_mix(rows, columns, position):
    x = rows.astype(F32)
    return (
        columns[:, 3:4]
        + shifted(x, 2, position) * columns[:, 0:1]
        + shifted(x, 1, position) * columns[:, 1:2]
        + x * columns[:, 2:3]
    )


def in_tiles(weight):
    rows, columns = weight.shape
    return weight.reshape(rows, columns // LANES, LANES).swapaxes(0, 1)


def body(
    stream,
    norm_gain,
    gate_weight,
    value_weight,
    gate_taps,
    value_taps,
    gate_bias,
    value_bias,
    down_weight,
    final_gain,
):
    batch_rows, length, width = stream.shape
    tokens = batch_rows * length
    ny, nx, nz = lax.axis_size("y"), lax.axis_size("x"), lax.axis_size("z")
    ff = gate_weight.shape[2]
    block = ff // ny
    units = block // nz
    half = block // 2
    core = lax.axis_index("dp")
    plane = ("y", "x")
    members = nx * ny
    piece = tokens // members
    position = lax.broadcasted_iota(jnp.int32, (1, tokens), 1) % length

    first = core == 0
    sent = [
        jnp.broadcast_to(stream.reshape(1, tokens, width), (ny, tokens, width)),
        jnp.broadcast_to(jnp.pad(norm_gain, ((0, 14), (0, 0)))[None], (ny, 16, width)),
    ]
    for layer in range(LAYERS):
        up = in_tiles(jnp.where(first, gate_weight[layer], value_weight[layer]))
        sent.append(up.reshape(ny, -1, LANES))
        down = down_weight[layer].reshape(ny, 2, half, width)
        sent.append(lax.dynamic_index_in_dim(down, core, 1, keepdims=False))
    ends, at = [], 0
    for a in sent[:-1]:
        at += a.shape[1]
        ends.append(at)
    mine = exchanged(jnp.concatenate(sent, axis=1), "y")
    other = lax.ppermute(mine, "dp", [(0, 1), (1, 0)])
    mine = jnp.split(mine, ends, axis=1)
    other = jnp.split(other, ends, axis=1)

    lower = lax.axis_index("y") * block + lax.axis_index("z") * units
    table = jnp.concatenate(
        [gate_taps, gate_bias[:, None], value_taps, value_bias[:, None]], axis=1
    )
    table = lax.dynamic_slice_in_dim(table, lower, units, 2)
    table = jnp.swapaxes(table, 1, 2).astype(F32)
    gains = mine[1].astype(F32)
    place = lax.axis_index(plane)

    current = mine[0]
    for layer in range(LAYERS):
        values = current.astype(F32)
        squares = jnp.sum(values * values, axis=(0, 2))[None]
        gained = (values * gains[:, layer][:, None]).astype(BF16)
        gained = gained.swapaxes(0, 1).reshape(tokens, ny * width)

        def projected(tiles):
            tiles = tiles.reshape(ny, block // LANES, width, LANES)
            weight = tiles.transpose(0, 2, 1, 3).reshape(ny * width, block)
            out = jnp.dot(gained, weight, preferred_element_type=F32).astype(BF16)
            return out.T.reshape(nz, units, tokens)

        a, b = projected(mine[2 + 2 * layer]), projected(other[2 + 2 * layer])
        parts = jnp.concatenate(
            [
                jnp.where(first, a, b),
                jnp.where(first, b, a),
                jnp.broadcast_to(jnp.pad(two_halves(squares), ((0, 6), (0, 0)))[None], (nz, 8, tokens)),
            ],
            axis=1,
        )
        total = exchanged(parts, "z").astype(F32).sum(axis=0)
        scale = lax.rsqrt((total[2 * units] + total[2 * units + 1])[None] / D + EPS)
        gate_up = (total[:units] * scale).astype(BF16)
        value_up = (total[units : 2 * units] * scale).astype(BF16)
        gate_conv = causal_mix(gate_up, table[layer, :, 0:4], position)
        value_conv = causal_mix(value_up, table[layer, :, 4:8], position)
        hidden = (jax.nn.gelu(gate_conv) * value_conv).astype(BF16)
        gathered = to_everyone(hidden, "z").reshape(2, half, tokens)
        down = (mine[3 + 2 * layer], other[3 + 2 * layer])
        term = 0.0
        for k in range(2):
            rows = lax.dynamic_index_in_dim(gathered, core if k == 0 else 1 - core, 0, keepdims=False)
            term = term + jnp.einsum("ut,yud->ytd", rows, down[k], preferred_element_type=F32)
        term = term.astype(BF16)
        if layer < LAYERS - 1:
            term = term.reshape(ny, members, piece, width).swapaxes(0, 1)
            summed = exchanged(term, plane).astype(F32).sum(axis=0)
            own = lax.dynamic_slice_in_dim(values, place * piece, piece, 1)
            fresh = (0.5 * own + summed).astype(BF16)
            current = to_everyone(fresh, plane).swapaxes(0, 1).reshape(ny, tokens, width)
        else:
            term = jnp.broadcast_to(term[:, None], (ny, nx, tokens, width)).reshape(members, tokens, width)
            branch = exchanged(term, plane).astype(F32).sum(axis=0)
            own = lax.dynamic_index_in_dim(values, lax.axis_index("y"), 0, keepdims=False)
            last = (0.5 * own + branch).astype(BF16).astype(F32)
    squares = jnp.sum(last * last, axis=1)[None]
    total = to_everyone(two_halves(squares), ("z", "y")).astype(F32).sum(axis=(0, 1))
    mixed = last * lax.rsqrt(total[:, None] / D + EPS) * final_gain.astype(F32)[None]
    return mixed.astype(BF16).reshape(batch_rows, length, width)


def solution(mesh):
    split = Mesh(
        mesh.devices.reshape(8, 4, mesh.shape["cb"], mesh.shape["dp"]), ("z", "y", "x", "dp")
    )
    ra = ("z", "y")
    return jax.shard_map(
        body,
        mesh=split,
        in_specs=(
            P("dp", None, ra),
            P(None, ra),
            P(None, ra, "x"),
            P(None, ra, "x"),
            P(None, None, "x"),
            P(None, None, "x"),
            P(None, "x"),
            P(None, "x"),
            P(None, "x", ra),
            P(ra),
        ),
        out_specs=P("dp", None, ra),
        check_vma=False,
    )
```

```python
import functools

import jax
import jax.numpy as jnp
from jax import lax
from jax.experimental import pallas as pl
from jax.experimental.pallas import tpu as pltpu
from jax.sharding import Mesh
from jax.sharding import PartitionSpec as P

D = 4096
LAYERS = 2
LANES = 128
EXTRA = 16
EPS = 1e-06
F32 = jnp.float32
BF16 = jnp.bfloat16
TN = (((0,), (0,)), ((), ()))
VMEM = pl.BlockSpec(memory_space=pltpu.VMEM)
ANY = pl.BlockSpec(memory_space=pl.ANY)


def exchanged(x, axis):
    return lax.all_to_all(x, axis, split_axis=0, concat_axis=0, tiled=True)


def to_everyone(x, axis):
    copies = jnp.broadcast_to(x[None], (lax.axis_size(axis), *x.shape))
    return exchanged(copies, axis)


def two_halves(row):
    high = row.astype(BF16)
    low = (row - high.astype(F32)).astype(BF16)
    return jnp.concatenate([high, low], axis=0)


def room(mebibytes):
    return pltpu.CompilerParams(vmem_limit_bytes=mebibytes * 1024 * 1024)


def cost(flops, moved):
    return pl.CostEstimate(flops=flops, bytes_accessed=moved, transcendentals=0)


def pack_kernel(layer, ny, start, *refs):
    if start:
        gate, value, stream, gain, out, sems = refs
    else:
        gate, value, out, sems = refs
    width = gate.shape[1]
    tiles = gate.shape[2] // LANES
    each = tiles // ny
    first = lax.axis_index("dp") == 0

    def copies(ref):
        for j in range(tiles):
            yield pltpu.make_async_copy(
                ref.at[layer, :, pl.ds(j * LANES, LANES)],
                out.at[j // each, pl.ds(start + (j % each) * width, width), :],
                sems.at[j],
            )

    @pl.when(first)
    def _():
        for c in copies(gate):
            c.start()

    @pl.when(jnp.logical_not(first))
    def _():
        for c in copies(value):
            c.start()

    if start:
        tokens = stream.shape[0]
        block = stream[...]
        gains = jnp.broadcast_to(gain[...].astype(F32)[:, None, :], (LAYERS, 8, width))
        gains = gains.reshape(LAYERS * 8, width).astype(BF16)
        for i in range(ny):
            out[i, 0:tokens, :] = block
            out[i, tokens : tokens + LAYERS * 8, :] = gains
    for c in copies(gate):
        c.wait()


def packed(layer, ny, gate, value, stream=None, gain=None):
    width, columns = gate.shape[1:]
    rows = columns // ny // LANES * width
    start = 0 if stream is None else stream.shape[0] + LAYERS * 8
    args = (gate, value) if stream is None else (gate, value, stream, gain)
    specs = [ANY, ANY] if stream is None else [ANY, ANY, VMEM, VMEM]
    return pl.pallas_call(
        functools.partial(pack_kernel, layer, ny, start),
        out_shape=jax.ShapeDtypeStruct((ny, start + rows, LANES), BF16),
        in_specs=specs,
        out_specs=VMEM,
        scratch_shapes=[pltpu.SemaphoreType.DMA((columns // LANES,))],
        cost_estimate=cost(1000000, 2 * width * columns * 2),
        compiler_params=room(4),
        name=f"pack{layer}",
    )(*args)


def up_kernel(layer, start, ny, nx, nz, *refs):
    if layer == 0:
        mine, other, out = refs
        first_mine = mine
        weights = [(mine.at[k], other.at[k]) for k in range(ny)]
    else:
        first_mine, terms = refs[0], refs[1]
        weights = [(refs[2 + k], refs[2 + ny + k]) for k in range(ny)]
        out, kept = refs[2 + 2 * ny :]
    tokens = LANES
    width = LANES
    block = weights[0][0].shape[0] - start
    units = block // nz
    core = lax.axis_index("dp")
    y = lax.axis_index("y")
    squares = jnp.zeros((tokens, LANES), F32)
    gained = []
    for k in range(ny):
        at = k if layer == 0 else lax.rem(y - k + ny, ny)
        values = first_mine[at, 0:tokens, :].astype(F32)
        if layer:
            branch = terms[at * nx].astype(F32)
            for i in range(1, nx):
                branch = branch + terms[at * nx + i].astype(F32)
            rounded = (0.5 * values + branch).astype(BF16)
            if k == 0:
                kept[...] = rounded
            values = rounded.astype(F32)
        gain = first_mine[at, tokens : tokens + 16, :].astype(F32)[8 * layer : 8 * layer + 1]
        squares = squares + values * values
        gained.append((values * gain).astype(BF16))
    gained = jnp.concatenate(gained, axis=1)
    for side in range(2):
        rows = pl.multiple_of((core if side == 0 else 1 - core) * units, 16)
        for j in range(block // LANES):
            weight = jnp.concatenate(
                [w[side][pl.ds(start + j * width, width), :] for w in weights], axis=0
            )
            result = jnp.dot(gained, weight, preferred_element_type=F32).T.astype(BF16)
            low = j * LANES
            while low < (j + 1) * LANES:
                slot = low // units
                high = min((j + 1) * LANES, (slot + 1) * units)
                out[slot, pl.ds(rows + (low - slot * units), high - low), :] = result[
                    low - j * LANES : high - j * LANES
                ]
                low = high
    total = jnp.broadcast_to(jnp.sum(squares, axis=1, keepdims=True), (tokens, LANES)).T[0:EXTRA]
    high = total.astype(BF16).astype(F32)
    index = lax.broadcasted_iota(jnp.int32, (EXTRA, LANES), 0)
    both = jnp.where(index == 0, high, jnp.where(index == 1, total - high, 0.0)).astype(BF16)
    for i in range(nz):
        out[i, 2 * units : 2 * units + EXTRA, :] = both


def projected(layer, start, block, ny, nx, nz, args):
    units = block // nz
    shapes = [jax.ShapeDtypeStruct((nz, 2 * units + EXTRA, LANES), BF16)]
    if layer:
        shapes.append(jax.ShapeDtypeStruct((LANES, LANES), BF16))
    return pl.pallas_call(
        functools.partial(up_kernel, layer, start, ny, nx, nz),
        out_shape=shapes,
        in_specs=[VMEM] * len(args),
        out_specs=[VMEM] * len(shapes),
        cost_estimate=cost(4 * ny * LANES * LANES * block, 4 * ny * LANES * block),
        compiler_params=room(8),
        name=f"up{layer}",
    )(*args)


def mid_kernel(length, parts, table, out):
    count, rows, tokens = parts.shape
    units = out.shape[1]
    total = parts[0].astype(F32)
    for i in range(1, count):
        total = total + parts[i].astype(F32)
    mean = (total[2 * units : 2 * units + 1] + total[2 * units + 1 : 2 * units + 2]) / D
    scale = lax.rsqrt(mean + EPS)
    position = lax.rem(lax.broadcasted_iota(jnp.int32, (units, tokens), 1), length)
    columns = table[...]

    def mixed(low, at):
        x = (total[low : low + units] * scale).astype(BF16).astype(F32)
        one = jnp.where(position >= 1, pltpu.roll(x, 1, 1), 0.0)
        two = jnp.where(position >= 2, pltpu.roll(x, 2, 1), 0.0)
        return (
            columns[:, at + 3 : at + 4]
            + two * columns[:, at : at + 1]
            + one * columns[:, at + 1 : at + 2]
            + x * columns[:, at + 2 : at + 3]
        )

    hidden = (jax.nn.gelu(mixed(0, 0)) * mixed(units, 4)).astype(BF16)
    for i in range(out.shape[0]):
        out[i] = hidden


def gated(parts, table, length, copies):
    units = table.shape[0]
    return pl.pallas_call(
        functools.partial(mid_kernel, length),
        out_shape=jax.ShapeDtypeStruct((copies, units, parts.shape[2]), BF16),
        in_specs=[VMEM] * 2,
        out_specs=VMEM,
        cost_estimate=cost(1000000, parts.size * 2),
        compiler_params=room(6),
        name="mid",
    )(parts, table)


def down_kernel(hidden, weight, out):
    term = lax.dot_general(hidden[...], weight[0], TN, preferred_element_type=F32).astype(BF16)
    for i in range(out.shape[0]):
        out[i] = term


def lowered(layer, hidden, weight, copies):
    rows, width = weight.shape[1:]
    return pl.pallas_call(
        down_kernel,
        grid=(1,),
        out_shape=jax.ShapeDtypeStruct((copies, hidden.shape[1], width), BF16),
        in_specs=[
            pl.BlockSpec((rows, hidden.shape[1]), lambda i: (0, 0)),
            pl.BlockSpec((1, rows, width), lambda i: (layer, 0, 0)),
        ],
        out_specs=pl.BlockSpec((copies, hidden.shape[1], width), lambda i: (0, 0, 0)),
        cost_estimate=cost(2 * rows * width * hidden.shape[1], 4 * rows * width),
        compiler_params=room(8),
        name=f"down{layer}",
    )(hidden, weight)


def body(
    stream,
    norm_gain,
    gate_weight,
    value_weight,
    gate_taps,
    value_taps,
    gate_bias,
    value_bias,
    down_weight,
    final_gain,
):
    batch_rows, length, width = stream.shape
    tokens = batch_rows * length
    ny, nx, nz = lax.axis_size("y"), lax.axis_size("x"), lax.axis_size("z")
    block = gate_weight.shape[2] // ny
    units = block // nz
    start = tokens + LAYERS * 8
    swap = [(0, 1), (1, 0)]
    own = stream.reshape(tokens, width)

    mine = exchanged(packed(0, ny, gate_weight, value_weight, own, norm_gain), "y")
    other = lax.ppermute(mine, "dp", swap)
    later, mine = lax.optimization_barrier((packed(1, ny, gate_weight, value_weight), mine))
    y = lax.axis_index("y")
    near, far = [], []
    for k in range(ny):
        piece = lax.dynamic_index_in_dim(later, lax.rem(y + k, ny), 0, keepdims=False)
        if k:
            piece = lax.ppermute(piece, "y", [(i, (i + k) % ny) for i in range(ny)])
        near.append(piece)

    lower = y * block + lax.axis_index("z") * units
    table = jnp.concatenate(
        [gate_taps, gate_bias[:, None], value_taps, value_bias[:, None]], axis=1
    )
    table = lax.dynamic_slice_in_dim(table, lower, units, 2)
    table = jnp.swapaxes(table, 1, 2).astype(F32)

    (parts,) = projected(0, start, block, ny, nx, nz, [mine, other])
    parts, *near = lax.optimization_barrier((exchanged(parts, "z"), *near))
    far = [lax.ppermute(piece, "dp", swap) for piece in near]
    hidden = gated(parts, table[0], length, nz * ny)
    hidden = exchanged(hidden, ("y", "z")).reshape(-1, tokens)
    terms = exchanged(lowered(0, hidden, down_weight, ny * nx), ("y", "x"))

    parts, kept = projected(1, 0, block, ny, nx, nz, [mine, terms, *near, *far])
    hidden = gated(exchanged(parts, "z"), table[1], length, nz * ny)
    hidden = exchanged(hidden, ("y", "z")).reshape(-1, tokens)
    terms = exchanged(lowered(1, hidden, down_weight, nx), "x")
    branch = terms.astype(F32).sum(axis=0)
    last = (0.5 * kept.astype(F32) + branch).astype(BF16).astype(F32)
    squares = jnp.sum(last * last, axis=1)[None]
    total = to_everyone(two_halves(squares), ("z", "y")).astype(F32).sum(axis=(0, 1))
    mixed = last * lax.rsqrt(total[:, None] / D + EPS) * final_gain.astype(F32)[None]
    return mixed.astype(BF16).reshape(batch_rows, length, width)


def solution(mesh):
    split = Mesh(
        mesh.devices.reshape(8, 4, mesh.shape["cb"], mesh.shape["dp"]), ("z", "y", "x", "dp")
    )
    ra = ("z", "y")
    return jax.shard_map(
        body,
        mesh=split,
        in_specs=(
            P("dp", None, ra),
            P(None, ra),
            P(None, ra, "x"),
            P(None, ra, "x"),
            P(None, None, "x"),
            P(None, None, "x"),
            P(None, "x"),
            P(None, "x"),
            P(None, "x", ra),
            P(ra),
        ),
        out_specs=P("dp", None, ra),
        check_vma=False,
    )
```

```python
import functools

import jax
import jax.numpy as jnp
from jax import lax
from jax.experimental import pallas as pl
from jax.experimental.pallas import tpu as pltpu
from jax.sharding import Mesh
from jax.sharding import PartitionSpec as P

D = 4096
LAYERS = 2
LANES = 128
EXTRA = 16
WHOLE_VMEM = 67043328
EPS = 1e-06
F32 = jnp.float32
BF16 = jnp.bfloat16
VMEM = pl.BlockSpec(memory_space=pltpu.VMEM)
HBM = pl.BlockSpec(memory_space=pltpu.MemorySpace.HBM)


def exchanged(x, axis):
    return lax.all_to_all(x, axis, split_axis=0, concat_axis=0, tiled=True)


def room(mebibytes):
    return pltpu.CompilerParams(vmem_limit_bytes=mebibytes * 1024 * 1024)


def cost(flops, moved):
    return pl.CostEstimate(flops=flops, bytes_accessed=moved, transcendentals=0)


def half_copies(up, down, layer, ny, core, at, out, start, sems, first):
    width, columns = up.shape[1:]
    each = columns // ny // LANES
    half = columns // ny // 2
    for j in range(each):
        low = pl.multiple_of((at * each + j) * LANES, LANES)
        yield pltpu.make_async_copy(
            up.at[layer, :, pl.ds(low, LANES)],
            out.at[pl.ds(start + j * width, width), :],
            sems.at[first + j],
        )
    low = pl.multiple_of((at * 2 + core) * half, half)
    yield pltpu.make_async_copy(
        down.at[layer, pl.ds(low, half), :],
        out.at[pl.ds(start + each * width, half), :],
        sems.at[first + each],
    )


def pack_first_kernel(ny, gate, value, down, stream, gain, out, held, sems, more):
    tokens, width = stream.shape
    each = gate.shape[2] // ny // LANES + 1
    start = tokens + LAYERS * 8
    core = lax.axis_index("dp")
    others = [
        pltpu.make_async_copy(stream, out.at[i, pl.ds(0, tokens), :], more.at[i]) for i in range(ny)
    ]
    others.append(pltpu.make_async_copy(gain, held, more.at[ny]))

    def copies(up):
        for i in range(ny):
            yield from half_copies(up, down, 0, ny, core, i, out.at[i], start, sems, i * each)

    @pl.when(core == 0)
    def _():
        for c in copies(gate):
            c.start()

    @pl.when(core == 1)
    def _():
        for c in copies(value):
            c.start()

    for c in others:
        c.start()
    others[-1].wait()
    gains = jnp.broadcast_to(held[...].astype(F32)[:, None, :], (LAYERS, 8, width))
    gains = gains.reshape(LAYERS * 8, width).astype(BF16)
    for i in range(ny):
        out[i, tokens : tokens + LAYERS * 8, :] = gains
    for c in others[:-1]:
        c.wait()
    for c in copies(gate):
        c.wait()


def packed_first(ny, gate, value, down, stream, gain):
    rows = gate.shape[1] * gate.shape[2] // ny // LANES + down.shape[1] // ny // 2
    rows += stream.shape[0] + LAYERS * 8
    each = gate.shape[2] // ny // LANES + 1
    return pl.pallas_call(
        functools.partial(pack_first_kernel, ny),
        out_shape=jax.ShapeDtypeStruct((ny, rows, LANES), BF16),
        in_specs=[HBM] * 5,
        out_specs=VMEM,
        scratch_shapes=[
            pltpu.VMEM(gain.shape, BF16),
            pltpu.SemaphoreType.DMA((ny * each,)),
            pltpu.SemaphoreType.DMA((ny + 1,)),
        ],
        cost_estimate=cost(1000000, 2 * ny * rows * LANES),
        compiler_params=pltpu.CompilerParams(
            vmem_limit_bytes=WHOLE_VMEM - 2 * ny * rows * LANES - 16384
        ),
        name="pack0",
    )(gate, value, down, stream, gain)


def pack_second_kernel(ny, gate, value, down, *refs):
    outs, sems = refs[:-1], refs[-1]
    each = gate.shape[2] // ny // LANES + 1
    core = lax.axis_index("dp")
    y = lax.axis_index("y")

    def copies(up, spare):
        for k in range(ny):
            at = lax.rem(y + k, ny)
            yield from half_copies(up, down, 1, ny, core, at, outs[k], 0, sems, k * each)
        yield from half_copies(spare, down, 1, ny, 1 - core, y, outs[ny], 0, sems, ny * each)

    @pl.when(core == 0)
    def _():
        for c in copies(gate, value):
            c.start()

    @pl.when(core == 1)
    def _():
        for c in copies(value, gate):
            c.start()

    for c in copies(gate, value):
        c.wait()


def packed_second(ny, gate, value, down):
    rows = gate.shape[1] * gate.shape[2] // ny // LANES + down.shape[1] // ny // 2
    each = gate.shape[2] // ny // LANES + 1
    return pl.pallas_call(
        functools.partial(pack_second_kernel, ny),
        out_shape=[jax.ShapeDtypeStruct((rows, LANES), BF16)] * (ny + 1),
        in_specs=[HBM] * 3,
        out_specs=[VMEM] * (ny + 1),
        scratch_shapes=[pltpu.SemaphoreType.DMA(((ny + 1) * each,))],
        cost_estimate=cost(1000000, 2 * ny * rows * LANES),
        compiler_params=pltpu.CompilerParams(vmem_limit_bytes=WHOLE_VMEM - 1490000),
        name="pack1",
    )(gate, value, down)


def high_and_low(squares):
    tokens = squares.shape[0]
    total = jnp.broadcast_to(jnp.sum(squares, axis=1, keepdims=True), (tokens, LANES)).T[0:EXTRA]
    high = total.astype(BF16).astype(F32)
    index = lax.broadcasted_iota(jnp.int32, (EXTRA, tokens), 0)
    return jnp.where(index == 0, high, jnp.where(index == 1, total - high, 0.0)).astype(BF16)


def up_kernel(layer, start, ny, nz, block, *refs):
    mine = refs[0]
    if layer == 0:
        weights = [(mine.at[k], refs[1].at[k]) for k in range(ny)]
        (out,) = refs[2:]
    else:
        fresh = refs[1]
        weights = [(refs[2 + k], refs[2 + ny + k]) for k in range(ny)]
        out, kept = refs[2 + 2 * ny :]
    tokens = LANES
    width = LANES
    units = block // nz
    core = lax.axis_index("dp")
    y = lax.axis_index("y")
    squares = jnp.zeros((tokens, LANES), F32)
    gained = []
    for k in range(ny):
        at = k if layer == 0 else lax.rem(y - k + ny, ny)
        if layer:
            values = fresh[:, at].astype(F32).reshape(tokens, width)
            if k == 0:
                kept[...] = values.astype(BF16)
        else:
            values = mine[at, 0:tokens, :].astype(F32)
        gain = mine[at, tokens : tokens + 16, :].astype(F32)[8 * layer : 8 * layer + 1]
        squares = squares + values * values
        gained.append((values * gain).astype(BF16))
    gained = jnp.concatenate(gained, axis=1)
    for side in range(2):
        rows = pl.multiple_of((core if side == 0 else 1 - core) * units, 16)
        for j in range(block // LANES):
            weight = jnp.concatenate(
                [w[side][pl.ds(start + j * width, width), :] for w in weights], axis=0
            )
            result = jnp.dot(gained, weight, preferred_element_type=F32).T.astype(BF16)
            low = j * LANES
            while low < (j + 1) * LANES:
                slot = low // units
                high = min((j + 1) * LANES, (slot + 1) * units)
                out[slot, pl.ds(rows + (low - slot * units), high - low), :] = result[
                    low - j * LANES : high - j * LANES
                ]
                low = high
    both = high_and_low(squares)
    for i in range(nz):
        out[i, 2 * units : 2 * units + EXTRA, :] = both


def projected(layer, start, block, ny, nz, args):
    units = block // nz
    shapes = [jax.ShapeDtypeStruct((nz, 2 * units + EXTRA, LANES), BF16)]
    if layer:
        shapes.append(jax.ShapeDtypeStruct((LANES, LANES), BF16))
    return pl.pallas_call(
        functools.partial(up_kernel, layer, start, ny, nz, block),
        out_shape=shapes,
        in_specs=[VMEM] * len(args),
        out_specs=[VMEM] * len(shapes),
        cost_estimate=cost(4 * ny * LANES * LANES * block, 4 * ny * LANES * block),
        compiler_params=room(8),
        name=f"up{layer}",
    )(*args)


def mid_kernel(length, parts, table, out):
    count, rows, tokens = parts.shape
    units = out.shape[1]
    total = parts[0].astype(F32)
    for i in range(1, count):
        total = total + parts[i].astype(F32)
    mean = (total[2 * units : 2 * units + 1] + total[2 * units + 1 : 2 * units + 2]) / D
    scale = lax.rsqrt(mean + EPS)
    position = lax.rem(lax.broadcasted_iota(jnp.int32, (units, tokens), 1), length)
    spread = jnp.concatenate([table[...]] * (LANES // 8), axis=0)
    columns = spread.T[0:units]

    def mixed(low, at):
        x = (total[low : low + units] * scale).astype(BF16).astype(F32)
        one = jnp.where(position >= 1, pltpu.roll(x, 1, 1), 0.0)
        two = jnp.where(position >= 2, pltpu.roll(x, 2, 1), 0.0)
        return (
            columns[:, at + 3 : at + 4]
            + two * columns[:, at : at + 1]
            + one * columns[:, at + 1 : at + 2]
            + x * columns[:, at + 2 : at + 3]
        )

    hidden = (jax.nn.gelu(mixed(0, 0)) * mixed(units, 4)).astype(BF16)
    for i in range(out.shape[0]):
        out[i] = hidden


def gated(parts, table, units, length):
    return pl.pallas_call(
        functools.partial(mid_kernel, length),
        out_shape=jax.ShapeDtypeStruct((parts.shape[0], units, parts.shape[2]), BF16),
        in_specs=[VMEM] * 2,
        out_specs=VMEM,
        cost_estimate=cost(1000000, parts.size * 2),
        compiler_params=room(6),
        name="mid",
    )(parts, table)


def down_kernel(layer, start, half, ny, nx, hidden, *refs):
    out = refs[-1]
    if layer == 0:
        sides = [[ref.at[k] for k in range(ny)] for ref in refs[:2]]
    else:
        sides = [refs[0:ny], refs[ny : 2 * ny]]
    nz, units, tokens = hidden.shape
    core = lax.axis_index("dp")
    y = lax.axis_index("y")
    term = 0.0
    for side, weights in enumerate(sides):
        first = (core if side == 0 else 1 - core) * (nz // 2)
        rows = hidden[pl.ds(first, nz // 2)].reshape(half, tokens).T
        weight = jnp.concatenate([w[pl.ds(start, half), :] for w in weights], axis=1)
        term = term + jnp.dot(rows, weight, preferred_element_type=F32)
    for k in range(ny):
        piece = term[:, k * LANES : (k + 1) * LANES]
        if layer == 0:
            out[:, k] = piece.reshape(ny * nx, -1, LANES).astype(BF16)
        else:
            at = lax.rem(y - k + ny, ny)
            for i in range(nx):
                out[at * nx + i] = piece.astype(BF16)


def lowered(layer, start, half, ny, nx, args):
    tokens = args[0].shape[2]
    count = ny * nx
    shape = (count, ny, tokens // count, LANES) if layer == 0 else (count, tokens, LANES)
    return pl.pallas_call(
        functools.partial(down_kernel, layer, start, half, ny, nx),
        out_shape=jax.ShapeDtypeStruct(shape, BF16),
        in_specs=[VMEM] * len(args),
        out_specs=VMEM,
        cost_estimate=cost(4 * half * ny * LANES * tokens, 4 * half * ny * LANES),
        compiler_params=room(8),
        name=f"down{layer}",
    )(*args)


def add_kernel(terms, mine, out):
    count, ny, piece, width = terms.shape
    place = lax.axis_index("y") * (count // ny) + lax.axis_index("x")
    total = terms[0].astype(F32)
    for i in range(1, count):
        total = total + terms[i].astype(F32)
    rows = pl.multiple_of(place * piece, piece)
    own = mine[:, pl.ds(rows, piece), :].astype(F32)
    fresh = (0.5 * own + total).astype(BF16)
    for i in range(count):
        out[i] = fresh


def added(terms, mine):
    return pl.pallas_call(
        add_kernel,
        out_shape=jax.ShapeDtypeStruct(terms.shape, BF16),
        in_specs=[VMEM] * 2,
        out_specs=VMEM,
        cost_estimate=cost(1000000, terms.size * 4),
        compiler_params=room(4),
        name="add",
    )(terms, mine)


def last_kernel(terms, kept, last, out):
    total = terms[0].astype(F32)
    for i in range(1, terms.shape[0]):
        total = total + terms[i].astype(F32)
    fresh = (0.5 * kept[...].astype(F32) + total).astype(BF16)
    last[...] = fresh
    values = fresh.astype(F32)
    both = high_and_low(values * values)
    for i in range(out.shape[0]):
        out[i] = both


def finished(terms, kept, copies):
    return pl.pallas_call(
        last_kernel,
        out_shape=[
            jax.ShapeDtypeStruct(kept.shape, BF16),
            jax.ShapeDtypeStruct((copies, EXTRA, terms.shape[1]), BF16),
        ],
        in_specs=[VMEM] * 2,
        out_specs=[VMEM] * 2,
        cost_estimate=cost(1000000, terms.size * 4),
        compiler_params=room(4),
        name="last",
    )(terms, kept)


def norm_kernel(last, parts, gain, out):
    tokens = last.shape[0]
    total = parts[0].astype(F32)
    for i in range(1, parts.shape[0]):
        total = total + parts[i].astype(F32)
    scale = lax.rsqrt((total[0:1] + total[1:2]) / D + EPS)
    column = jnp.broadcast_to(scale, (LANES, tokens)).T
    values = last[...].astype(F32) * column * gain[...].astype(F32)
    out[...] = values.astype(BF16)


def normed(last, parts, gain):
    return pl.pallas_call(
        norm_kernel,
        out_shape=jax.ShapeDtypeStruct(last.shape, BF16),
        in_specs=[VMEM] * 3,
        out_specs=VMEM,
        cost_estimate=cost(1000000, last.size * 4),
        compiler_params=room(4),
        name="norm",
    )(last, parts, gain)


def body(
    stream,
    norm_gain,
    gate_weight,
    value_weight,
    gate_taps,
    value_taps,
    gate_bias,
    value_bias,
    down_weight,
    final_gain,
):
    batch_rows, length, width = stream.shape
    tokens = batch_rows * length
    ny, nx, nz = lax.axis_size("y"), lax.axis_size("x"), lax.axis_size("z")
    block = gate_weight.shape[2] // ny
    half = block // 2
    units = block // nz
    start = tokens + LAYERS * 8
    swap = [(0, 1), (1, 0)]
    own = stream.reshape(tokens, width)

    mine = exchanged(packed_first(ny, gate_weight, value_weight, down_weight, own, norm_gain), "y")
    other = lax.ppermute(mine, "dp", swap)
    later = packed_second(ny, gate_weight, value_weight, down_weight)
    *later, mine = lax.optimization_barrier((*later, mine))
    near = [later[0]]
    for k in range(1, ny):
        near.append(lax.ppermute(later[k], "y", [(i, (i + k) % ny) for i in range(ny)]))

    lower = lax.axis_index("y") * block + lax.axis_index("z") * units
    table = jnp.concatenate(
        [gate_taps, gate_bias[:, None], value_taps, value_bias[:, None]], axis=1
    )
    table = lax.dynamic_slice_in_dim(table, lower, units, 2).astype(F32)
    table = jnp.pad(table, ((0, 0), (0, 0), (0, LANES - units)))

    (parts,) = projected(0, start, block, ny, nz, [mine, other])
    hidden = exchanged(gated(exchanged(parts, "z"), table[0], units, length), "z")
    terms = lowered(0, start + block, half, ny, nx, [hidden, mine, other])
    terms = exchanged(terms, ("y", "x"))
    fresh = exchanged(added(terms, mine), ("y", "x"))
    far = [later[ny]] + [lax.ppermute(piece, "dp", swap) for piece in near[1:]]

    parts, kept = projected(1, 0, block, ny, nz, [mine, fresh, *near, *far])
    hidden = exchanged(gated(exchanged(parts, "z"), table[1], units, length), "z")
    terms = exchanged(lowered(1, block, half, ny, nx, [hidden, *near, *far]), ("y", "x"))
    last, squares = finished(terms, kept, nz * ny)
    squares = exchanged(squares, ("z", "y"))
    mixed = normed(last, squares, final_gain[None])
    return mixed.reshape(batch_rows, length, width)


def solution(mesh):
    split = Mesh(
        mesh.devices.reshape(8, 4, mesh.shape["cb"], mesh.shape["dp"]), ("z", "y", "x", "dp")
    )
    ra = ("z", "y")
    return jax.shard_map(
        body,
        mesh=split,
        in_specs=(
            P("dp", None, ra),
            P(None, ra),
            P(None, ra, "x"),
            P(None, ra, "x"),
            P(None, None, "x"),
            P(None, None, "x"),
            P(None, "x"),
            P(None, "x"),
            P(None, "x", ra),
            P(ra),
        ),
        out_specs=P("dp", None, ra),
        check_vma=False,
    )
```

```python
import functools

import jax
import jax.numpy as jnp
from jax import lax
from jax.experimental import pallas as pl
from jax.experimental.pallas import tpu as pltpu
from jax.sharding import Mesh
from jax.sharding import PartitionSpec as P


D = 4096
LAYERS = 2
LANES = 128
EXTRA = 16
WHOLE_VMEM = 67043328
EPS = 1e-06
F32 = jnp.float32
BF16 = jnp.bfloat16
VMEM = pl.BlockSpec(memory_space=pltpu.VMEM)
HBM = pl.BlockSpec(memory_space=pltpu.MemorySpace.HBM)


def exchanged(x, axis):
    return lax.all_to_all(x, axis, split_axis=0, concat_axis=0, tiled=True)


def room(mebibytes):
    return pltpu.CompilerParams(vmem_limit_bytes=mebibytes * 1024 * 1024)


def cost(flops, moved):
    return pl.CostEstimate(flops=flops, bytes_accessed=moved, transcendentals=0)


def up_copies(up, layer, ny, at, out, start, sems, first):
    width, columns = up.shape[1:]
    each = columns // ny // LANES
    for j in range(each):
        low = pl.multiple_of((at * each + j) * LANES, LANES)
        yield pltpu.make_async_copy(
            up.at[layer, :, pl.ds(low, LANES)],
            out.at[pl.ds(start + j * width, width), :],
            sems.at[first + j],
        )


def down_copies(down, ny, core, at, out, start, sems, first):
    half = down.shape[1] // ny // 2
    low = pl.multiple_of((at * 2 + core) * half, half)
    for layer in range(LAYERS):
        yield pltpu.make_async_copy(
            down.at[layer, pl.ds(low, half), :],
            out.at[pl.ds(start + layer * half, half), :],
            sems.at[first + layer],
        )


def pack_first_kernel(ny, gate, value, stream, gain, out, held, sems, more):
    tokens, width = stream.shape
    each = gate.shape[2] // ny // LANES
    start = tokens + LAYERS * 8
    core = lax.axis_index("dp")
    others = [
        pltpu.make_async_copy(stream, out.at[i, pl.ds(0, tokens), :], more.at[i]) for i in range(ny)
    ]
    others.append(pltpu.make_async_copy(gain, held, more.at[ny]))

    def copies(up):
        for i in range(ny):
            yield from up_copies(up, 0, ny, i, out.at[i], start, sems, i * each)

    @pl.when(core == 0)
    def _():
        for c in copies(gate):
            c.start()

    @pl.when(core == 1)
    def _():
        for c in copies(value):
            c.start()

    for c in others:
        c.start()
    others[-1].wait()
    gains = jnp.broadcast_to(held[...].astype(F32)[:, None, :], (LAYERS, 8, width))
    gains = gains.reshape(LAYERS * 8, width).astype(BF16)
    for i in range(ny):
        out[i, tokens : tokens + LAYERS * 8, :] = gains
    for c in others[:-1]:
        c.wait()
    for c in copies(gate):
        c.wait()


def packed_first(ny, gate, value, stream, gain):
    rows = gate.shape[1] * gate.shape[2] // ny // LANES
    rows += stream.shape[0] + LAYERS * 8
    each = gate.shape[2] // ny // LANES
    return pl.pallas_call(
        functools.partial(pack_first_kernel, ny),
        out_shape=jax.ShapeDtypeStruct((ny, rows, LANES), BF16),
        in_specs=[HBM] * 4,
        out_specs=VMEM,
        scratch_shapes=[
            pltpu.VMEM(gain.shape, BF16),
            pltpu.SemaphoreType.DMA((ny * each,)),
            pltpu.SemaphoreType.DMA((ny + 1,)),
        ],
        cost_estimate=cost(1000000, 2 * ny * rows * LANES),
        compiler_params=pltpu.CompilerParams(
            vmem_limit_bytes=WHOLE_VMEM - 2 * ny * rows * LANES - 16384
        ),
        name="pack0",
    )(gate, value, stream, gain)


def pack_second_kernel(ny, gate, value, down, *refs):
    outs, sems = refs[:-1], refs[-1]
    ups = gate.shape[2] // ny // LANES
    rows = ups * gate.shape[1]
    each = ups + LAYERS
    core = lax.axis_index("dp")
    y = lax.axis_index("y")

    def copies(up, spare):
        for k in range(ny + 1):
            at = lax.rem(y + k, ny) if k < ny else y
            side = core if k < ny else 1 - core
            first = k * each
            yield from up_copies(up if k < ny else spare, 1, ny, at, outs[k], 0, sems, first)
            yield from down_copies(down, ny, side, at, outs[k], rows, sems, first + ups)

    @pl.when(core == 0)
    def _():
        for c in copies(gate, value):
            c.start()

    @pl.when(core == 1)
    def _():
        for c in copies(value, gate):
            c.start()

    for c in copies(gate, value):
        c.wait()


def packed_second(ny, gate, value, down):
    rows = gate.shape[1] * gate.shape[2] // ny // LANES + LAYERS * down.shape[1] // ny // 2
    each = gate.shape[2] // ny // LANES + LAYERS
    return pl.pallas_call(
        functools.partial(pack_second_kernel, ny),
        out_shape=[jax.ShapeDtypeStruct((rows, LANES), BF16)] * (ny + 1),
        in_specs=[HBM] * 3,
        out_specs=[VMEM] * (ny + 1),
        scratch_shapes=[pltpu.SemaphoreType.DMA(((ny + 1) * each,))],
        cost_estimate=cost(1000000, 2 * ny * rows * LANES),
        compiler_params=room(4),
        name="pack1",
    )(gate, value, down)


def high_and_low(squares):
    tokens = squares.shape[0]
    total = jnp.broadcast_to(jnp.sum(squares, axis=1, keepdims=True), (tokens, LANES)).T[0:EXTRA]
    high = total.astype(BF16).astype(F32)
    index = lax.broadcasted_iota(jnp.int32, (EXTRA, tokens), 0)
    return jnp.where(index == 0, high, jnp.where(index == 1, total - high, 0.0)).astype(BF16)


def up_kernel(layer, start, ny, nz, block, *refs):
    mine = refs[0]
    if layer == 0:
        weights = [(mine.at[k], refs[1].at[k]) for k in range(ny)]
        (out,) = refs[2:]
    else:
        fresh = refs[1]
        weights = [(refs[2 + k], refs[2 + ny + k]) for k in range(ny)]
        out, kept = refs[2 + 2 * ny :]
    tokens = LANES
    width = LANES
    units = block // nz
    core = lax.axis_index("dp")
    y = lax.axis_index("y")
    squares = jnp.zeros((tokens, LANES), F32)
    gained = []
    for k in range(ny):
        at = k if layer == 0 else lax.rem(y - k + ny, ny)
        if layer:
            values = fresh[:, at].astype(F32).reshape(tokens, width)
            if k == 0:
                kept[...] = values.astype(BF16)
        else:
            values = mine[at, 0:tokens, :].astype(F32)
        gain = mine[at, tokens : tokens + 16, :].astype(F32)[8 * layer : 8 * layer + 1]
        squares = squares + values * values
        gained.append((values * gain).astype(BF16))
    gained = jnp.concatenate(gained, axis=1)
    for side in range(2):
        rows = pl.multiple_of((core if side == 0 else 1 - core) * units, 16)
        for j in range(block // LANES):
            weight = jnp.concatenate(
                [w[side][pl.ds(start + j * width, width), :] for w in weights], axis=0
            )
            result = jnp.dot(gained, weight, preferred_element_type=F32).T.astype(BF16)
            low = j * LANES
            while low < (j + 1) * LANES:
                slot = low // units
                high = min((j + 1) * LANES, (slot + 1) * units)
                out[slot, pl.ds(rows + (low - slot * units), high - low), :] = result[
                    low - j * LANES : high - j * LANES
                ]
                low = high
    both = high_and_low(squares)
    for i in range(nz):
        out[i, 2 * units : 2 * units + EXTRA, :] = both


def projected(layer, start, block, ny, nz, args):
    units = block // nz
    shapes = [jax.ShapeDtypeStruct((nz, 2 * units + EXTRA, LANES), BF16)]
    if layer:
        shapes.append(jax.ShapeDtypeStruct((LANES, LANES), BF16))
    return pl.pallas_call(
        functools.partial(up_kernel, layer, start, ny, nz, block),
        out_shape=shapes,
        in_specs=[VMEM] * len(args),
        out_specs=[VMEM] * len(shapes),
        cost_estimate=cost(4 * ny * LANES * LANES * block, 4 * ny * LANES * block),
        compiler_params=room(8),
    )(*args)


def mid_kernel(length, parts, table, out):
    count, _, tokens = parts.shape
    units = out.shape[1]
    total = parts[0].astype(F32)
    for i in range(1, count):
        total = total + parts[i].astype(F32)
    mean = (total[2 * units : 2 * units + 1] + total[2 * units + 1 : 2 * units + 2]) / D
    scale = lax.rsqrt(mean + EPS)
    position = lax.rem(lax.broadcasted_iota(jnp.int32, (units, tokens), 1), length)
    spread = jnp.concatenate([table[...]] * (LANES // 8), axis=0)
    columns = spread.T[0:units]

    def mixed(low, at):
        x = (total[low : low + units] * scale).astype(BF16).astype(F32)
        one = jnp.where(position >= 1, pltpu.roll(x, 1, 1), 0.0)
        two = jnp.where(position >= 2, pltpu.roll(x, 2, 1), 0.0)
        return (
            columns[:, at + 3 : at + 4]
            + two * columns[:, at : at + 1]
            + one * columns[:, at + 1 : at + 2]
            + x * columns[:, at + 2 : at + 3]
        )

    hidden = (jax.nn.gelu(mixed(0, 0)) * mixed(units, 4)).astype(BF16)
    for i in range(out.shape[0]):
        out[i] = hidden


def gated(parts, table, units, length):
    return pl.pallas_call(
        functools.partial(mid_kernel, length),
        out_shape=jax.ShapeDtypeStruct((parts.shape[0], units, parts.shape[2]), BF16),
        in_specs=[VMEM] * 2,
        out_specs=VMEM,
        cost_estimate=cost(1000000, parts.size * 2),
        compiler_params=room(6),
        name="mid",
    )(parts, table)


def down_kernel(layer, start, half, ny, nx, hidden, *refs):
    out = refs[-1]
    sides = [refs[0:ny], refs[ny : 2 * ny]]
    nz, _, tokens = hidden.shape
    core = lax.axis_index("dp")
    y = lax.axis_index("y")
    term = 0.0
    for side, weights in enumerate(sides):
        first = (core if side == 0 else 1 - core) * (nz // 2)
        rows = hidden[pl.ds(first, nz // 2)].reshape(half, tokens).T
        weight = jnp.concatenate([w[pl.ds(start, half), :] for w in weights], axis=1)
        term = term + jnp.dot(rows, weight, preferred_element_type=F32)
    for k in range(ny):
        piece = term[:, k * LANES : (k + 1) * LANES]
        at = lax.rem(y - k + ny, ny)
        if layer == 0:
            out[:, at] = piece.reshape(ny * nx, -1, LANES).astype(BF16)
        else:
            for i in range(nx):
                out[at * nx + i] = piece.astype(BF16)


def lowered(layer, start, half, ny, nx, args):
    tokens = args[0].shape[2]
    count = ny * nx
    shape = (count, ny, tokens // count, LANES) if layer == 0 else (count, tokens, LANES)
    return pl.pallas_call(
        functools.partial(down_kernel, layer, start, half, ny, nx),
        out_shape=jax.ShapeDtypeStruct(shape, BF16),
        in_specs=[VMEM] * len(args),
        out_specs=VMEM,
        cost_estimate=cost(4 * half * ny * LANES * tokens, 4 * half * ny * LANES),
        compiler_params=room(8),
    )(*args)


def add_kernel(terms, mine, out):
    count, ny, piece, _ = terms.shape
    place = lax.axis_index("y") * (count // ny) + lax.axis_index("x")
    total = terms[0].astype(F32)
    for i in range(1, count):
        total = total + terms[i].astype(F32)
    rows = pl.multiple_of(place * piece, piece)
    own = mine[:, pl.ds(rows, piece), :].astype(F32)
    fresh = (0.5 * own + total).astype(BF16)
    for i in range(count):
        out[i] = fresh


def added(terms, mine):
    return pl.pallas_call(
        add_kernel,
        out_shape=jax.ShapeDtypeStruct(terms.shape, BF16),
        in_specs=[VMEM] * 2,
        out_specs=VMEM,
        cost_estimate=cost(1000000, terms.size * 4),
        compiler_params=room(4),
        name="add",
    )(terms, mine)


def last_kernel(terms, kept, last, out):
    total = terms[0].astype(F32)
    for i in range(1, terms.shape[0]):
        total = total + terms[i].astype(F32)
    fresh = (0.5 * kept[...].astype(F32) + total).astype(BF16)
    last[...] = fresh
    values = fresh.astype(F32)
    both = high_and_low(values * values)
    for i in range(out.shape[0]):
        out[i] = both


def finished(terms, kept, copies):
    return pl.pallas_call(
        last_kernel,
        out_shape=[
            jax.ShapeDtypeStruct(kept.shape, BF16),
            jax.ShapeDtypeStruct((copies, EXTRA, terms.shape[1]), BF16),
        ],
        in_specs=[VMEM] * 2,
        out_specs=[VMEM] * 2,
        cost_estimate=cost(1000000, terms.size * 4),
        compiler_params=room(4),
        name="last",
    )(terms, kept)


def norm_kernel(last, parts, gain, out):
    tokens = last.shape[0]
    total = parts[0].astype(F32)
    for i in range(1, parts.shape[0]):
        total = total + parts[i].astype(F32)
    scale = lax.rsqrt((total[0:1] + total[1:2]) / D + EPS)
    column = jnp.broadcast_to(scale, (LANES, tokens)).T
    values = last[...].astype(F32) * column * gain[...].astype(F32)
    out[...] = values.astype(BF16)


def normed(last, parts, gain):
    return pl.pallas_call(
        norm_kernel,
        out_shape=jax.ShapeDtypeStruct(last.shape, BF16),
        in_specs=[VMEM] * 3,
        out_specs=VMEM,
        cost_estimate=cost(1000000, last.size * 4),
        compiler_params=room(4),
        name="norm",
    )(last, parts, gain)


def layers(
    stream,
    norm_gain,
    gate_weight,
    value_weight,
    gate_taps,
    value_taps,
    gate_bias,
    value_bias,
    down_weight,
    final_gain,
):
    batch_rows, length, width = stream.shape
    tokens = batch_rows * length
    ny, nx, nz = lax.axis_size("y"), lax.axis_size("x"), lax.axis_size("z")
    block = gate_weight.shape[2] // ny
    half = block // 2
    units = block // nz
    start = tokens + LAYERS * 8
    swap = [(0, 1), (1, 0)]
    own = stream.reshape(tokens, width)

    mine = packed_first(ny, gate_weight, value_weight, own, norm_gain)
    mine = exchanged(mine, "y")
    other = lax.ppermute(mine, "dp", swap)
    (parts,) = projected(0, start, block, ny, nz, [mine, other])
    parts = exchanged(parts, "z")

    later = packed_second(ny, gate_weight, value_weight, down_weight)
    near = [later[0]]
    for k in range(1, ny):
        near.append(lax.ppermute(later[k], "y", [(i, (i + k) % ny) for i in range(ny)]))

    lower = lax.axis_index("y") * block + lax.axis_index("z") * units
    table = jnp.concatenate(
        [gate_taps, gate_bias[:, None], value_taps, value_bias[:, None]], axis=1
    )
    table = lax.dynamic_slice_in_dim(table, lower, units, 2).astype(F32)
    table = jnp.pad(table, ((0, 0), (0, 0), (0, LANES - units)))

    hidden = gated(parts, table[0], units, length)
    hidden = exchanged(hidden, "z")
    far = [later[ny]] + [lax.ppermute(piece, "dp", swap) for piece in near[1:]]
    terms = lowered(0, block, half, ny, nx, [hidden, *near, *far])
    terms = exchanged(terms, ("y", "x"))
    fresh = exchanged(added(terms, mine), ("y", "x"))

    parts, kept = projected(1, 0, block, ny, nz, [mine, fresh, *near, *far])
    hidden = exchanged(gated(exchanged(parts, "z"), table[1], units, length), "z")
    terms = lowered(1, block + half, half, ny, nx, [hidden, *near, *far])
    terms = exchanged(terms, ("y", "x"))
    last, squares = finished(terms, kept, nz * ny)
    squares = exchanged(squares, ("z", "y"))
    mixed = normed(last, squares, final_gain[None])
    return mixed.reshape(batch_rows, length, width)


def solution(mesh):
    split = Mesh(
        mesh.devices.reshape(8, 4, mesh.shape["cb"], mesh.shape["dp"]), ("z", "y", "x", "dp")
    )
    ra = ("z", "y")
    return jax.shard_map(
        layers,
        mesh=split,
        in_specs=(
            P("dp", None, ra),
            P(None, ra),
            P(None, ra, "x"),
            P(None, ra, "x"),
            P(None, None, "x"),
            P(None, None, "x"),
            P(None, "x"),
            P(None, "x"),
            P(None, "x", ra),
            P(ra),
        ),
        out_specs=P("dp", None, ra),
        check_vma=False,
    )
```

```python
import functools

import jax
import jax.numpy as jnp
from jax import lax
from jax.experimental import pallas as pl
from jax.experimental.pallas import tpu as pltpu
from jax.sharding import Mesh
from jax.sharding import PartitionSpec as P


D = 4096
LAYERS = 2
LANES = 128
EXTRA = 8
WHOLE_VMEM = 67043328
EPS = 1e-06
F32 = jnp.float32
BF16 = jnp.bfloat16
VMEM = pl.BlockSpec(memory_space=pltpu.VMEM)
HBM = pl.BlockSpec(memory_space=pltpu.MemorySpace.HBM)


def exchanged(x, axis):
    return lax.all_to_all(x, axis, split_axis=0, concat_axis=0, tiled=True)


def room(mebibytes):
    return pltpu.CompilerParams(vmem_limit_bytes=mebibytes * 1024 * 1024)


def cost(flops, moved):
    return pl.CostEstimate(flops=flops, bytes_accessed=moved, transcendentals=0)


def up_copies(up, layer, ny, at, out, start, sems, first):
    width, columns = up.shape[1:]
    each = columns // ny // LANES
    for j in range(each):
        low = pl.multiple_of((at * each + j) * LANES, LANES)
        yield pltpu.make_async_copy(
            up.at[layer, :, pl.ds(low, LANES)],
            out.at[pl.ds(start + j * width, width), :],
            sems.at[first + j],
        )


def down_copies(down, ny, core, at, out, start, sems, first):
    half = down.shape[1] // ny // 2
    low = pl.multiple_of((at * 2 + core) * half, half)
    for layer in range(LAYERS):
        yield pltpu.make_async_copy(
            down.at[layer, pl.ds(low, half), :],
            out.at[pl.ds(start + layer * half, half), :],
            sems.at[first + layer],
        )


def pack_first_kernel(ny, gate, value, stream, gain, out, held, sems, more):
    tokens, width = stream.shape
    each = gate.shape[2] // ny // LANES
    start = tokens + LAYERS * 8
    copies = []
    for i in range(ny):
        first = 2 * i * each
        second = first + each
        copies.extend(up_copies(gate, 0, ny, i, out.at[i], start, sems, first))
        copies.extend(up_copies(value, 0, ny, i, out.at[i], start + each * width, sems, second))
        copies.append(
            pltpu.make_async_copy(stream, out.at[i, pl.ds(0, tokens), :], more.at[i])
        )
    gains = pltpu.make_async_copy(gain, held, more.at[ny])
    gains.start()
    for c in copies:
        c.start()
    gains.wait()
    gains = jnp.broadcast_to(held[...].astype(F32)[:, None, :], (LAYERS, 8, width))
    gains = gains.reshape(LAYERS * 8, width).astype(BF16)
    for i in range(ny):
        out[i, tokens : tokens + LAYERS * 8, :] = gains
    for c in copies:
        c.wait()


def packed_first(ny, gate, value, stream, gain):
    each = gate.shape[2] // ny // LANES
    rows = 2 * each * gate.shape[1] + stream.shape[0] + LAYERS * 8
    return pl.pallas_call(
        functools.partial(pack_first_kernel, ny),
        out_shape=jax.ShapeDtypeStruct((ny, rows, LANES), BF16),
        in_specs=[HBM] * 4,
        out_specs=VMEM,
        scratch_shapes=[
            pltpu.VMEM(gain.shape, BF16),
            pltpu.SemaphoreType.DMA((2 * ny * each,)),
            pltpu.SemaphoreType.DMA((ny + 1,)),
        ],
        cost_estimate=cost(1000000, 2 * ny * rows * LANES),
        compiler_params=pltpu.CompilerParams(vmem_limit_bytes=WHOLE_VMEM - 950000),
        name="pack0",
    )(gate, value, stream, gain)


def pack_second_kernel(ny, gate, value, down, *refs):
    outs, sems = refs[:-1], refs[-1]
    ups = gate.shape[2] // ny // LANES
    rows = ups * gate.shape[1]
    each = ups + LAYERS
    core = lax.axis_index("dp")
    y = lax.axis_index("y")

    def copies(up, spare):
        for k in range(ny + 1):
            at = lax.rem(y + k, ny) if k < ny else y
            side = core if k < ny else 1 - core
            first = k * each
            yield from up_copies(up if k < ny else spare, 1, ny, at, outs[k], 0, sems, first)
            yield from down_copies(down, ny, side, at, outs[k], rows, sems, first + ups)

    @pl.when(core == 0)
    def _():
        for c in copies(gate, value):
            c.start()

    @pl.when(core == 1)
    def _():
        for c in copies(value, gate):
            c.start()

    for c in copies(gate, value):
        c.wait()


def packed_second(ny, gate, value, down):
    rows = gate.shape[1] * gate.shape[2] // ny // LANES + LAYERS * down.shape[1] // ny // 2
    each = gate.shape[2] // ny // LANES + LAYERS
    return pl.pallas_call(
        functools.partial(pack_second_kernel, ny),
        out_shape=[jax.ShapeDtypeStruct((rows, LANES), BF16)] * (ny + 1),
        in_specs=[HBM] * 3,
        out_specs=[VMEM] * (ny + 1),
        scratch_shapes=[pltpu.SemaphoreType.DMA(((ny + 1) * each,))],
        cost_estimate=cost(1000000, 2 * ny * rows * LANES),
        compiler_params=room(4),
        name="pack1",
    )(gate, value, down)


def high_and_low(squares):
    tokens = squares.shape[0]
    total = jnp.broadcast_to(jnp.sum(squares, axis=1, keepdims=True), (tokens, LANES)).T[0:EXTRA]
    high = total.astype(BF16).astype(F32)
    index = lax.broadcasted_iota(jnp.int32, (EXTRA, tokens), 0)
    return jnp.where(index == 0, high, jnp.where(index == 1, total - high, 0.0)).astype(BF16)


def multiplied(gained, weights, start, block, store):
    width = LANES
    wide = 2 * LANES
    for j in range(block // wide):
        weight = jnp.concatenate(
            [
                jnp.concatenate(
                    [w[pl.ds(start + (2 * j + i) * width, width), :] for i in range(2)], axis=1
                )
                for w in weights
            ],
            axis=0,
        )
        store(j * wide, jnp.dot(gained, weight, preferred_element_type=F32).T.astype(BF16))


def into_slots(out, rows, units):
    def store(first, result):
        low, end = first, first + result.shape[0]
        while low < end:
            slot = low // units
            high = min(end, (slot + 1) * units)
            out[slot, pl.ds(rows + (low - slot * units), high - low), :] = result[
                low - first : high - first
            ]
            low = high

    return store


def with_gain(values, gain_block, layer):
    return (values * gain_block.astype(F32)[8 * layer : 8 * layer + 1]).astype(BF16)


def first_up_kernel(start, ny, nz, block, mine, out, state):
    tokens = LANES
    units = block // nz
    squares = jnp.zeros((tokens, LANES), F32)
    gained = []
    for k in range(ny):
        values = mine[k, 0:tokens, :].astype(F32)
        squares = squares + values * values
        gained.append(with_gain(values, mine[k, tokens : tokens + 16, :], 0))
    gained = jnp.concatenate(gained, axis=1)
    weights = [mine.at[k] for k in range(ny)]
    multiplied(gained, weights, start, block, into_slots(out, 0, units))
    multiplied(gained, weights, start + block, block, into_slots(out, units, units))
    both = high_and_low(squares)
    state[...] = mine[:, 0:start, :]
    for i in range(nz):
        out[i, 2 * units : 2 * units + EXTRA, :] = both


def first_projected(start, block, ny, nz, mine):
    units = block // nz
    return pl.pallas_call(
        functools.partial(first_up_kernel, start, ny, nz, block),
        out_shape=[
            jax.ShapeDtypeStruct((nz, 2 * units + EXTRA, LANES), BF16),
            jax.ShapeDtypeStruct((ny, start, LANES), BF16),
        ],
        in_specs=[VMEM],
        out_specs=[VMEM] * 2,
        cost_estimate=cost(4 * ny * LANES * LANES * block, 4 * ny * LANES * block),
        compiler_params=room(8),
        name="up0",
    )(mine)


def second_up_kernel(ny, nz, block, *refs):
    mine, fresh = refs[:2]
    sides = [refs[2 : 2 + ny], refs[2 + ny : 2 + 2 * ny]]
    out, kept = refs[2 + 2 * ny :]
    tokens = LANES
    units = block // nz
    core = lax.axis_index("dp")
    y = lax.axis_index("y")
    squares = jnp.zeros((tokens, LANES), F32)
    gained = []
    for k in range(ny):
        at = lax.rem(y - k + ny, ny)
        values = fresh[:, at].astype(F32).reshape(tokens, LANES)
        if k == 0:
            kept[...] = values.astype(BF16)
        squares = squares + values * values
        gained.append(with_gain(values, mine[at, tokens : tokens + 16, :], 1))
    gained = jnp.concatenate(gained, axis=1)
    for side, weights in enumerate(sides):
        rows = pl.multiple_of((core if side == 0 else 1 - core) * units, 16)
        multiplied(gained, weights, 0, block, into_slots(out, rows, units))
    both = high_and_low(squares)
    for i in range(nz):
        out[i, 2 * units : 2 * units + EXTRA, :] = both


def second_projected(block, ny, nz, args):
    units = block // nz
    return pl.pallas_call(
        functools.partial(second_up_kernel, ny, nz, block),
        out_shape=[
            jax.ShapeDtypeStruct((nz, 2 * units + EXTRA, LANES), BF16),
            jax.ShapeDtypeStruct((LANES, LANES), BF16),
        ],
        in_specs=[VMEM] * len(args),
        out_specs=[VMEM] * 2,
        cost_estimate=cost(4 * ny * LANES * LANES * block, 4 * ny * LANES * block),
        compiler_params=room(8),
        name="up1",
    )(*args)


def mid_kernel(layer, length, parts, table, out):
    count, _, tokens = parts.shape
    units = out.shape[1]
    total = parts[0].astype(F32)
    for i in range(1, count):
        total = total + parts[i].astype(F32)
    mean = (total[2 * units : 2 * units + 1] + total[2 * units + 1 : 2 * units + 2]) / D
    scale = lax.rsqrt(mean + EPS)
    position = lax.rem(lax.broadcasted_iota(jnp.int32, (units, tokens), 1), length)
    spread = jnp.concatenate([table[layer]] * (LANES // 8), axis=0)
    columns = spread.T[0:units]

    def mixed(low, at):
        x = (total[low : low + units] * scale).astype(BF16).astype(F32)
        one = jnp.where(position >= 1, pltpu.roll(x, 1, 1), 0.0)
        two = jnp.where(position >= 2, pltpu.roll(x, 2, 1), 0.0)
        return (
            columns[:, at + 3 : at + 4]
            + two * columns[:, at : at + 1]
            + one * columns[:, at + 1 : at + 2]
            + x * columns[:, at + 2 : at + 3]
        )

    hidden = (jax.nn.gelu(mixed(0, 0)) * mixed(units, 4)).astype(BF16)
    for i in range(out.shape[0]):
        out[i] = hidden


def gated(layer, parts, table, units, length):
    return pl.pallas_call(
        functools.partial(mid_kernel, layer, length),
        out_shape=jax.ShapeDtypeStruct((parts.shape[0], units, parts.shape[2]), BF16),
        in_specs=[VMEM] * 2,
        out_specs=VMEM,
        cost_estimate=cost(1000000, parts.size * 2),
        compiler_params=room(6),
    )(parts, table)


def down_kernel(layer, start, half, ny, nx, hidden, *refs):
    out = refs[-1]
    sides = [refs[0:ny], refs[ny : 2 * ny]]
    nz, _, tokens = hidden.shape
    core = lax.axis_index("dp")
    y = lax.axis_index("y")
    term = 0.0
    for side, weights in enumerate(sides):
        first = (core if side == 0 else 1 - core) * (nz // 2)
        rows = hidden[pl.ds(first, nz // 2)].reshape(half, tokens).T
        weight = jnp.concatenate([w[pl.ds(start, half), :] for w in weights], axis=1)
        term = term + jnp.dot(rows, weight, preferred_element_type=F32)
    for k in range(ny):
        piece = term[:, k * LANES : (k + 1) * LANES]
        at = lax.rem(y - k + ny, ny)
        if layer == 0:
            out[:, at] = piece.reshape(ny * nx, -1, LANES).astype(BF16)
        else:
            for i in range(nx):
                out[at * nx + i] = piece.astype(BF16)


def lowered(layer, start, half, ny, nx, args):
    tokens = args[0].shape[2]
    count = ny * nx
    shape = (count, ny, tokens // count, LANES) if layer == 0 else (count, tokens, LANES)
    return pl.pallas_call(
        functools.partial(down_kernel, layer, start, half, ny, nx),
        out_shape=jax.ShapeDtypeStruct(shape, BF16),
        in_specs=[VMEM] * len(args),
        out_specs=VMEM,
        cost_estimate=cost(4 * half * ny * LANES * tokens, 4 * half * ny * LANES),
        compiler_params=room(8),
    )(*args)


def add_kernel(terms, mine, out):
    count, ny, piece, _ = terms.shape
    place = lax.axis_index("y") * (count // ny) + lax.axis_index("x")
    total = terms[0].astype(F32)
    for i in range(1, count):
        total = total + terms[i].astype(F32)
    rows = pl.multiple_of(place * piece, piece)
    own = mine[:, pl.ds(rows, piece), :].astype(F32)
    fresh = (0.5 * own + total).astype(BF16)
    for i in range(count):
        out[i] = fresh


def added(terms, mine):
    return pl.pallas_call(
        add_kernel,
        out_shape=jax.ShapeDtypeStruct(terms.shape, BF16),
        in_specs=[VMEM] * 2,
        out_specs=VMEM,
        cost_estimate=cost(1000000, terms.size * 4),
        compiler_params=room(4),
        name="add",
    )(terms, mine)


def last_kernel(terms, kept, last, out):
    total = terms[0].astype(F32)
    for i in range(1, terms.shape[0]):
        total = total + terms[i].astype(F32)
    fresh = (0.5 * kept[...].astype(F32) + total).astype(BF16)
    last[...] = fresh
    values = fresh.astype(F32)
    both = high_and_low(values * values)
    for i in range(out.shape[0]):
        out[i] = both


def finished(terms, kept, copies):
    return pl.pallas_call(
        last_kernel,
        out_shape=[
            jax.ShapeDtypeStruct(kept.shape, BF16),
            jax.ShapeDtypeStruct((copies, EXTRA, terms.shape[1]), BF16),
        ],
        in_specs=[VMEM] * 2,
        out_specs=[VMEM] * 2,
        cost_estimate=cost(1000000, terms.size * 4),
        compiler_params=room(4),
        name="last",
    )(terms, kept)


def norm_kernel(last, parts, gain, out):
    tokens = last.shape[0]
    total = parts[0].astype(F32)
    for i in range(1, parts.shape[0]):
        total = total + parts[i].astype(F32)
    scale = lax.rsqrt((total[0:1] + total[1:2]) / D + EPS)
    column = jnp.broadcast_to(scale, (LANES, tokens)).T
    values = last[...].astype(F32) * column * gain[...].astype(F32)
    out[...] = values.astype(BF16)


def normed(last, parts, gain):
    return pl.pallas_call(
        norm_kernel,
        out_shape=jax.ShapeDtypeStruct(last.shape, BF16),
        in_specs=[VMEM] * 3,
        out_specs=VMEM,
        cost_estimate=cost(1000000, last.size * 4),
        compiler_params=room(4),
        name="norm",
    )(last, parts, gain)


def layers(
    stream,
    norm_gain,
    gate_weight,
    value_weight,
    gate_taps,
    value_taps,
    gate_bias,
    value_bias,
    down_weight,
    final_gain,
):
    batch_rows, length, width = stream.shape
    tokens = batch_rows * length
    ny, nx, nz = lax.axis_size("y"), lax.axis_size("x"), lax.axis_size("z")
    block = gate_weight.shape[2] // ny
    half = block // 2
    units = block // nz
    start = tokens + LAYERS * 8
    swap = [(0, 1), (1, 0)]
    own = stream.reshape(tokens, width)

    mine = packed_first(ny, gate_weight, value_weight, own, norm_gain)
    mine = exchanged(mine, "y")
    parts, state = first_projected(start, block, ny, nz, mine)
    parts = exchanged(parts, "z")

    later = packed_second(ny, gate_weight, value_weight, down_weight)
    near = [later[0]]
    for k in range(1, ny):
        near.append(lax.ppermute(later[k], "y", [(i, (i + k) % ny) for i in range(ny)]))

    lower = lax.axis_index("y") * block + lax.axis_index("z") * units
    table = jnp.concatenate(
        [gate_taps, gate_bias[:, None], value_taps, value_bias[:, None]], axis=1
    )
    table = lax.dynamic_slice_in_dim(table, lower, units, 2).astype(F32)
    table = jnp.pad(table, ((0, 0), (0, 0), (0, LANES - units)))

    hidden = gated(0, parts, table, units, length)
    hidden = exchanged(hidden, "z")
    far = [later[ny]] + [lax.ppermute(piece, "dp", swap) for piece in near[1:]]
    terms = lowered(0, block, half, ny, nx, [hidden, *near, *far])
    terms = exchanged(terms, ("y", "x"))
    fresh = exchanged(added(terms, state), ("y", "x"))

    parts, kept = second_projected(block, ny, nz, [state, fresh, *near, *far])
    hidden = exchanged(gated(1, exchanged(parts, "z"), table, units, length), "z")
    terms = lowered(1, block + half, half, ny, nx, [hidden, *near, *far])
    terms = exchanged(terms, ("y", "x"))
    last, squares = finished(terms, kept, nz * ny)
    squares = exchanged(squares, ("z", "y"))
    mixed = normed(last, squares, final_gain[None])
    return mixed.reshape(batch_rows, length, width)


def solution(mesh):
    split = Mesh(
        mesh.devices.reshape(8, 4, mesh.shape["cb"], mesh.shape["dp"]), ("z", "y", "x", "dp")
    )
    ra = ("z", "y")
    return jax.shard_map(
        layers,
        mesh=split,
        in_specs=(
            P("dp", None, ra),
            P(None, ra),
            P(None, ra, "x"),
            P(None, ra, "x"),
            P(None, None, "x"),
            P(None, None, "x"),
            P(None, "x"),
            P(None, "x"),
            P(None, "x", ra),
            P(ra),
        ),
        out_specs=P("dp", None, ra),
        check_vma=False,
    )
```

```python
import functools

import jax
import jax.numpy as jnp
from jax import lax
from jax.experimental import pallas as pl
from jax.experimental.pallas import tpu as pltpu
from jax.sharding import Mesh
from jax.sharding import PartitionSpec as P


D = 4096
LAYERS = 2
LANES = 128
EXTRA = 8
WHOLE_VMEM = 67043328
EPS = 1e-06
F32 = jnp.float32
BF16 = jnp.bfloat16
VMEM = pl.BlockSpec(memory_space=pltpu.VMEM)
HBM = pl.BlockSpec(memory_space=pltpu.MemorySpace.HBM)


def exchanged(x, axis):
    return lax.all_to_all(x, axis, split_axis=0, concat_axis=0, tiled=True)


def room(mebibytes):
    return pltpu.CompilerParams(vmem_limit_bytes=mebibytes * 1024 * 1024)


def cost(flops, moved):
    return pl.CostEstimate(flops=flops, bytes_accessed=moved, transcendentals=0)


def up_copies(up, layer, ny, at, out, start, sems, first):
    width, columns = up.shape[1:]
    each = columns // ny // LANES
    for j in range(each):
        low = pl.multiple_of((at * each + j) * LANES, LANES)
        yield pltpu.make_async_copy(
            up.at[layer, :, pl.ds(low, LANES)],
            out.at[pl.ds(start + j * width, width), :],
            sems.at[first + j],
        )


def down_copies(down, ny, core, at, out, start, sems, first):
    half = down.shape[1] // ny // 2
    low = pl.multiple_of((at * 2 + core) * half, half)
    for layer in range(LAYERS):
        yield pltpu.make_async_copy(
            down.at[layer, pl.ds(low, half), :],
            out.at[pl.ds(start + layer * half, half), :],
            sems.at[first + layer],
        )


def pack_first_kernel(ny, gate, value, stream, gain, out, held, sems, more):
    tokens, width = stream.shape
    each = gate.shape[2] // ny // LANES
    start = tokens + LAYERS * 8
    core = lax.axis_index("dp")
    others = [
        pltpu.make_async_copy(stream, out.at[i, pl.ds(0, tokens), :], more.at[i]) for i in range(ny)
    ]
    others.append(pltpu.make_async_copy(gain, held, more.at[ny]))

    def copies(up):
        for i in range(ny):
            yield from up_copies(up, 0, ny, i, out.at[i], start, sems, i * each)

    @pl.when(core == 0)
    def _():
        for c in copies(gate):
            c.start()

    @pl.when(core == 1)
    def _():
        for c in copies(value):
            c.start()

    for c in others:
        c.start()
    others[-1].wait()
    gains = jnp.broadcast_to(held[...].astype(F32)[:, None, :], (LAYERS, 8, width))
    gains = gains.reshape(LAYERS * 8, width).astype(BF16)
    for i in range(ny):
        out[i, tokens : tokens + LAYERS * 8, :] = gains
    for c in others[:-1]:
        c.wait()
    for c in copies(gate):
        c.wait()


def packed_first(ny, gate, value, stream, gain):
    rows = gate.shape[1] * gate.shape[2] // ny // LANES
    rows += stream.shape[0] + LAYERS * 8
    each = gate.shape[2] // ny // LANES
    return pl.pallas_call(
        functools.partial(pack_first_kernel, ny),
        out_shape=jax.ShapeDtypeStruct((ny, rows, LANES), BF16),
        in_specs=[HBM] * 4,
        out_specs=VMEM,
        scratch_shapes=[
            pltpu.VMEM(gain.shape, BF16),
            pltpu.SemaphoreType.DMA((ny * each,)),
            pltpu.SemaphoreType.DMA((ny + 1,)),
        ],
        cost_estimate=cost(1000000, 2 * ny * rows * LANES),
        compiler_params=pltpu.CompilerParams(
            vmem_limit_bytes=WHOLE_VMEM - 2 * ny * rows * LANES - 16384
        ),
        name="pack0",
    )(gate, value, stream, gain)


def pack_second_kernel(ny, gate, value, down, *refs):
    outs, sems = refs[:-1], refs[-1]
    ups = gate.shape[2] // ny // LANES
    each = ups + LAYERS
    core = lax.axis_index("dp")
    y = lax.axis_index("y")

    def copies(up, spare):
        for k in range(ny + 1):
            at = lax.rem(y + k, ny) if k < ny else y
            side = core if k < ny else 1 - core
            first = k * each
            yield from up_copies(up if k < ny else spare, 1, ny, at, outs[k], 0, sems, first)
            low = outs[ny + 1 + k]
            yield from down_copies(down, ny, side, at, low, 0, sems, first + ups)

    @pl.when(core == 0)
    def _():
        for c in copies(gate, value):
            c.start()

    @pl.when(core == 1)
    def _():
        for c in copies(value, gate):
            c.start()

    for c in copies(gate, value):
        c.wait()


def packed_second(ny, gate, value, down):
    rows = gate.shape[1] * gate.shape[2] // ny // LANES
    low = LAYERS * down.shape[1] // ny // 2
    each = gate.shape[2] // ny // LANES + LAYERS
    return pl.pallas_call(
        functools.partial(pack_second_kernel, ny),
        out_shape=[jax.ShapeDtypeStruct((rows, LANES), BF16)] * (ny + 1)
        + [jax.ShapeDtypeStruct((low, LANES), BF16)] * (ny + 1),
        in_specs=[HBM] * 3,
        out_specs=[VMEM] * (2 * ny + 2),
        scratch_shapes=[pltpu.SemaphoreType.DMA(((ny + 1) * each,))],
        cost_estimate=cost(1000000, 2 * ny * rows * LANES),
        compiler_params=room(4),
        name="pack1",
    )(gate, value, down)


def high_and_low(squares):
    tokens = squares.shape[0]
    total = jnp.broadcast_to(jnp.sum(squares, axis=1, keepdims=True), (tokens, LANES)).T[0:EXTRA]
    high = total.astype(BF16).astype(F32)
    index = lax.broadcasted_iota(jnp.int32, (EXTRA, tokens), 0)
    return jnp.where(index == 0, high, jnp.where(index == 1, total - high, 0.0)).astype(BF16)


def multiplied(gained, weights, start, block, store):
    width = LANES
    wide = 2 * LANES
    for j in range(block // wide):
        weight = jnp.concatenate(
            [
                jnp.concatenate(
                    [w[pl.ds(start + (2 * j + i) * width, width), :] for i in range(2)], axis=1
                )
                for w in weights
            ],
            axis=0,
        )
        store(j * wide, jnp.dot(gained, weight, preferred_element_type=F32).T.astype(BF16))


def into_slots(out, rows, units):
    def store(first, result):
        low, end = first, first + result.shape[0]
        while low < end:
            slot = low // units
            high = min(end, (slot + 1) * units)
            out[slot, pl.ds(rows + (low - slot * units), high - low), :] = result[
                low - first : high - first
            ]
            low = high

    return store


def with_gain(values, gain_block, layer):
    return (values * gain_block.astype(F32)[8 * layer : 8 * layer + 1]).astype(BF16)


def first_up_kernel(side, start, ny, nz, block, *refs):
    mine = refs[0]
    out = refs[1] if side == 0 else refs[3]
    tokens = LANES
    units = block // nz
    core = lax.axis_index("dp")
    gained = jnp.concatenate(
        [
            with_gain(mine[k, 0:tokens, :].astype(F32), mine[k, tokens : tokens + 16, :], 0)
            for k in range(ny)
        ],
        axis=1,
    )
    if side == 0:
        weights = [mine.at[k] for k in range(ny)]
        multiplied(gained, weights, start, block, into_slots(out, 0, units))
        return
    other, near = refs[1], refs[2]
    weights = [other.at[k] for k in range(ny)]
    rows = pl.multiple_of((1 - core) * units, 16)
    multiplied(gained, weights, start, block, into_slots(out, rows, units))
    squares = jnp.zeros((tokens, LANES), F32)
    for k in range(ny):
        values = mine[k, 0:tokens, :].astype(F32)
        squares = squares + values * values
    both = high_and_low(squares)
    rows = pl.multiple_of(core * units, 16)
    refs[4][...] = mine[:, 0:start, :]
    for i in range(nz):
        out[i, pl.ds(rows, units), :] = near[i]
        out[i, 2 * units : 2 * units + EXTRA, :] = both


def first_projected(side, start, block, ny, nz, args):
    units = block // nz
    rows = units if side == 0 else 2 * units + EXTRA
    shapes = [jax.ShapeDtypeStruct((nz, rows, LANES), BF16)]
    if side:
        shapes.append(jax.ShapeDtypeStruct((ny, start, LANES), BF16))
    return pl.pallas_call(
        functools.partial(first_up_kernel, side, start, ny, nz, block),
        out_shape=shapes,
        in_specs=[VMEM] * len(args),
        out_specs=[VMEM] * len(shapes),
        cost_estimate=cost(2 * ny * LANES * LANES * block, 2 * ny * LANES * block),
        compiler_params=room(8),
    )(*args)


def second_up_kernel(ny, nz, block, *refs):
    mine, fresh = refs[:2]
    sides = [refs[2 : 2 + ny], refs[2 + ny : 2 + 2 * ny]]
    out, kept = refs[2 + 2 * ny :]
    tokens = LANES
    units = block // nz
    core = lax.axis_index("dp")
    y = lax.axis_index("y")
    squares = jnp.zeros((tokens, LANES), F32)
    gained = []
    for k in range(ny):
        at = lax.rem(y - k + ny, ny)
        values = fresh[:, at].astype(F32).reshape(tokens, LANES)
        if k == 0:
            kept[...] = values.astype(BF16)
        squares = squares + values * values
        gained.append(with_gain(values, mine[at, tokens : tokens + 16, :], 1))
    gained = jnp.concatenate(gained, axis=1)
    for side, weights in enumerate(sides):
        rows = pl.multiple_of((core if side == 0 else 1 - core) * units, 16)
        multiplied(gained, weights, 0, block, into_slots(out, rows, units))
    both = high_and_low(squares)
    for i in range(nz):
        out[i, 2 * units : 2 * units + EXTRA, :] = both


def second_projected(block, ny, nz, args):
    units = block // nz
    return pl.pallas_call(
        functools.partial(second_up_kernel, ny, nz, block),
        out_shape=[
            jax.ShapeDtypeStruct((nz, 2 * units + EXTRA, LANES), BF16),
            jax.ShapeDtypeStruct((LANES, LANES), BF16),
        ],
        in_specs=[VMEM] * len(args),
        out_specs=[VMEM] * 2,
        cost_estimate=cost(4 * ny * LANES * LANES * block, 4 * ny * LANES * block),
        compiler_params=room(8),
        name="up1",
    )(*args)


def mid_kernel(layer, length, parts, table, out):
    count, _, tokens = parts.shape
    units = out.shape[1]
    total = parts[0].astype(F32)
    for i in range(1, count):
        total = total + parts[i].astype(F32)
    mean = (total[2 * units : 2 * units + 1] + total[2 * units + 1 : 2 * units + 2]) / D
    scale = lax.rsqrt(mean + EPS)
    position = lax.rem(lax.broadcasted_iota(jnp.int32, (units, tokens), 1), length)
    spread = jnp.concatenate([table[layer]] * (LANES // 8), axis=0)
    columns = spread.T[0:units]

    def mixed(low, at):
        x = (total[low : low + units] * scale).astype(BF16).astype(F32)
        one = jnp.where(position >= 1, pltpu.roll(x, 1, 1), 0.0)
        two = jnp.where(position >= 2, pltpu.roll(x, 2, 1), 0.0)
        return (
            columns[:, at + 3 : at + 4]
            + two * columns[:, at : at + 1]
            + one * columns[:, at + 1 : at + 2]
            + x * columns[:, at + 2 : at + 3]
        )

    hidden = (jax.nn.gelu(mixed(0, 0)) * mixed(units, 4)).astype(BF16)
    for i in range(out.shape[0]):
        out[i] = hidden


def gated(layer, parts, table, units, length):
    return pl.pallas_call(
        functools.partial(mid_kernel, layer, length),
        out_shape=jax.ShapeDtypeStruct((parts.shape[0], units, parts.shape[2]), BF16),
        in_specs=[VMEM] * 2,
        out_specs=VMEM,
        cost_estimate=cost(1000000, parts.size * 2),
        compiler_params=room(6),
    )(parts, table)


def down_kernel(layer, start, half, ny, nx, hidden, *refs):
    out = refs[-1]
    sides = [refs[0:ny], refs[ny : 2 * ny]]
    nz, _, tokens = hidden.shape
    core = lax.axis_index("dp")
    y = lax.axis_index("y")
    term = 0.0
    for side, weights in enumerate(sides):
        first = (core if side == 0 else 1 - core) * (nz // 2)
        rows = hidden[pl.ds(first, nz // 2)].reshape(half, tokens).T
        weight = jnp.concatenate([w[pl.ds(start, half), :] for w in weights], axis=1)
        term = term + jnp.dot(rows, weight, preferred_element_type=F32)
    for k in range(ny):
        piece = term[:, k * LANES : (k + 1) * LANES]
        at = lax.rem(y - k + ny, ny)
        if layer == 0:
            out[:, at] = piece.reshape(ny * nx, -1, LANES).astype(BF16)
        else:
            for i in range(nx):
                out[at * nx + i] = piece.astype(BF16)


def lowered(layer, start, half, ny, nx, args):
    tokens = args[0].shape[2]
    count = ny * nx
    shape = (count, ny, tokens // count, LANES) if layer == 0 else (count, tokens, LANES)
    return pl.pallas_call(
        functools.partial(down_kernel, layer, start, half, ny, nx),
        out_shape=jax.ShapeDtypeStruct(shape, BF16),
        in_specs=[VMEM] * len(args),
        out_specs=VMEM,
        cost_estimate=cost(4 * half * ny * LANES * tokens, 4 * half * ny * LANES),
        compiler_params=room(8),
    )(*args)


def add_kernel(terms, mine, out):
    count, ny, piece, _ = terms.shape
    place = lax.axis_index("y") * (count // ny) + lax.axis_index("x")
    total = terms[0].astype(F32)
    for i in range(1, count):
        total = total + terms[i].astype(F32)
    rows = pl.multiple_of(place * piece, piece)
    own = mine[:, pl.ds(rows, piece), :].astype(F32)
    fresh = (0.5 * own + total).astype(BF16)
    for i in range(count):
        out[i] = fresh


def added(terms, mine):
    return pl.pallas_call(
        add_kernel,
        out_shape=jax.ShapeDtypeStruct(terms.shape, BF16),
        in_specs=[VMEM] * 2,
        out_specs=VMEM,
        cost_estimate=cost(1000000, terms.size * 4),
        compiler_params=room(4),
        name="add",
    )(terms, mine)


def last_kernel(terms, kept, last, out):
    total = terms[0].astype(F32)
    for i in range(1, terms.shape[0]):
        total = total + terms[i].astype(F32)
    fresh = (0.5 * kept[...].astype(F32) + total).astype(BF16)
    last[...] = fresh
    values = fresh.astype(F32)
    both = high_and_low(values * values)
    for i in range(out.shape[0]):
        out[i] = both


def finished(terms, kept, copies):
    return pl.pallas_call(
        last_kernel,
        out_shape=[
            jax.ShapeDtypeStruct(kept.shape, BF16),
            jax.ShapeDtypeStruct((copies, EXTRA, terms.shape[1]), BF16),
        ],
        in_specs=[VMEM] * 2,
        out_specs=[VMEM] * 2,
        cost_estimate=cost(1000000, terms.size * 4),
        compiler_params=room(4),
        name="last",
    )(terms, kept)


def norm_kernel(last, parts, gain, out):
    tokens = last.shape[0]
    total = parts[0].astype(F32)
    for i in range(1, parts.shape[0]):
        total = total + parts[i].astype(F32)
    scale = lax.rsqrt((total[0:1] + total[1:2]) / D + EPS)
    column = jnp.broadcast_to(scale, (LANES, tokens)).T
    values = last[...].astype(F32) * column * gain[...].astype(F32)
    out[...] = values.astype(BF16)


def normed(last, parts, gain):
    return pl.pallas_call(
        norm_kernel,
        out_shape=jax.ShapeDtypeStruct(last.shape, BF16),
        in_specs=[VMEM] * 3,
        out_specs=VMEM,
        cost_estimate=cost(1000000, last.size * 4),
        compiler_params=room(4),
        name="norm",
    )(last, parts, gain)


def layers(
    stream,
    norm_gain,
    gate_weight,
    value_weight,
    gate_taps,
    value_taps,
    gate_bias,
    value_bias,
    down_weight,
    final_gain,
):
    batch_rows, length, width = stream.shape
    tokens = batch_rows * length
    ny, nx, nz = lax.axis_size("y"), lax.axis_size("x"), lax.axis_size("z")
    block = gate_weight.shape[2] // ny
    half = block // 2
    units = block // nz
    start = tokens + LAYERS * 8
    swap = [(0, 1), (1, 0)]
    own = stream.reshape(tokens, width)

    mine = packed_first(ny, gate_weight, value_weight, own, norm_gain)
    mine = exchanged(mine, "y")
    other = lax.ppermute(mine, "dp", swap)
    (parts,) = first_projected(0, start, block, ny, nz, [mine])
    parts, state = first_projected(1, start, block, ny, nz, [mine, other, parts])
    parts = exchanged(parts, "z")

    later = packed_second(ny, gate_weight, value_weight, down_weight)
    ups, downs = later[: ny + 1], later[ny + 1 :]
    turns = [[(i, (i + k) % ny) for i in range(ny)] for k in range(ny)]
    near_down, near_up = [downs[0]], [ups[0]]
    for k in range(1, ny):
        near_down.append(lax.ppermute(downs[k], "y", turns[k]))
        near_up.append(lax.ppermute(ups[k], "y", turns[k]))

    lower = lax.axis_index("y") * block + lax.axis_index("z") * units
    table = jnp.concatenate(
        [gate_taps, gate_bias[:, None], value_taps, value_bias[:, None]], axis=1
    )
    table = lax.dynamic_slice_in_dim(table, lower, units, 2).astype(F32)
    table = jnp.pad(table, ((0, 0), (0, 0), (0, LANES - units)))

    hidden = gated(0, parts, table, units, length)
    hidden = exchanged(hidden, "z")
    far_down = [downs[ny]] + [lax.ppermute(piece, "dp", swap) for piece in near_down[1:]]
    lows = [*near_down, *far_down]
    terms = lowered(0, 0, half, ny, nx, [hidden, *lows])
    terms = exchanged(terms, ("y", "x"))
    far_up = [ups[ny]] + [lax.ppermute(piece, "dp", swap) for piece in near_up[1:]]
    fresh = exchanged(added(terms, state), ("y", "x"))

    parts, kept = second_projected(block, ny, nz, [state, fresh, *near_up, *far_up])
    hidden = exchanged(gated(1, exchanged(parts, "z"), table, units, length), "z")
    terms = lowered(1, half, half, ny, nx, [hidden, *lows])
    terms = exchanged(terms, ("y", "x"))
    last, squares = finished(terms, kept, nz * ny)
    squares = exchanged(squares, ("z", "y"))
    mixed = normed(last, squares, final_gain[None])
    return mixed.reshape(batch_rows, length, width)


def solution(mesh):
    split = Mesh(
        mesh.devices.reshape(8, 4, mesh.shape["cb"], mesh.shape["dp"]), ("z", "y", "x", "dp")
    )
    ra = ("z", "y")
    return jax.shard_map(
        layers,
        mesh=split,
        in_specs=(
            P("dp", None, ra),
            P(None, ra),
            P(None, ra, "x"),
            P(None, ra, "x"),
            P(None, None, "x"),
            P(None, None, "x"),
            P(None, "x"),
            P(None, "x"),
            P(None, "x", ra),
            P(ra),
        ),
        out_specs=P("dp", None, ra),
        check_vma=False,
    )
```

```python
import functools

import jax
import jax.numpy as jnp
from jax import lax
from jax.experimental import pallas as pl
from jax.experimental.pallas import tpu as pltpu
from jax.sharding import Mesh
from jax.sharding import PartitionSpec as P


D = 4096
LAYERS = 2
LANES = 128
EXTRA = 8
WHOLE_VMEM = 67043328
EPS = 1e-06
F32 = jnp.float32
BF16 = jnp.bfloat16
VMEM = pl.BlockSpec(memory_space=pltpu.VMEM)
HBM = pl.BlockSpec(memory_space=pltpu.MemorySpace.HBM)


def exchanged(x, axis):
    return lax.all_to_all(x, axis, split_axis=0, concat_axis=0, tiled=True)


def room(mebibytes):
    return pltpu.CompilerParams(vmem_limit_bytes=mebibytes * 1024 * 1024)


def cost(flops, moved):
    return pl.CostEstimate(flops=flops, bytes_accessed=moved, transcendentals=0)


def up_copies(up, layer, ny, at, out, start, sems, first):
    width, columns = up.shape[1:]
    each = columns // ny // LANES
    for j in range(each):
        low = pl.multiple_of((at * each + j) * LANES, LANES)
        yield pltpu.make_async_copy(
            up.at[layer, :, pl.ds(low, LANES)],
            out.at[pl.ds(start + j * width, width), :],
            sems.at[first + j],
        )


def down_copies(down, ny, core, at, out, start, sems, first):
    half = down.shape[1] // ny // 2
    low = pl.multiple_of((at * 2 + core) * half, half)
    for layer in range(LAYERS):
        yield pltpu.make_async_copy(
            down.at[layer, pl.ds(low, half), :],
            out.at[pl.ds(start + layer * half, half), :],
            sems.at[first + layer],
        )


def pack_first_kernel(ny, gate, value, stream, gain, out, held, sems, more):
    tokens, width = stream.shape
    each = gate.shape[2] // ny // LANES
    start = tokens + LAYERS * 8
    core = lax.axis_index("dp")
    others = [
        pltpu.make_async_copy(stream, out.at[i, pl.ds(0, tokens), :], more.at[i]) for i in range(ny)
    ]
    others.append(pltpu.make_async_copy(gain, held, more.at[ny]))

    def copies(up):
        for i in range(ny):
            yield from up_copies(up, 0, ny, i, out.at[i], start, sems, i * each)

    @pl.when(core == 0)
    def _():
        for c in copies(gate):
            c.start()

    @pl.when(core == 1)
    def _():
        for c in copies(value):
            c.start()

    for c in others:
        c.start()
    others[-1].wait()
    gains = jnp.broadcast_to(held[...].astype(F32)[:, None, :], (LAYERS, 8, width))
    gains = gains.reshape(LAYERS * 8, width).astype(BF16)
    for i in range(ny):
        out[i, tokens : tokens + LAYERS * 8, :] = gains
    for c in others[:-1]:
        c.wait()
    for c in copies(gate):
        c.wait()


def packed_first(ny, gate, value, stream, gain):
    rows = gate.shape[1] * gate.shape[2] // ny // LANES
    rows += stream.shape[0] + LAYERS * 8
    each = gate.shape[2] // ny // LANES
    return pl.pallas_call(
        functools.partial(pack_first_kernel, ny),
        out_shape=jax.ShapeDtypeStruct((ny, rows, LANES), BF16),
        in_specs=[HBM] * 4,
        out_specs=VMEM,
        scratch_shapes=[
            pltpu.VMEM(gain.shape, BF16),
            pltpu.SemaphoreType.DMA((ny * each,)),
            pltpu.SemaphoreType.DMA((ny + 1,)),
        ],
        cost_estimate=cost(1000000, 2 * ny * rows * LANES),
        compiler_params=pltpu.CompilerParams(
            vmem_limit_bytes=WHOLE_VMEM - 2 * ny * rows * LANES - 16384
        ),
        name="pack0",
    )(gate, value, stream, gain)


def pack_second_kernel(ny, gate, value, down, *refs):
    outs, sems = refs[:-1], refs[-1]
    ups = gate.shape[2] // ny // LANES
    rows = ups * gate.shape[1]
    each = ups + LAYERS
    core = lax.axis_index("dp")
    y = lax.axis_index("y")

    def copies(up, spare):
        for k in range(ny + 1):
            at = lax.rem(y + k, ny) if k < ny else y
            side = core if k < ny else 1 - core
            first = k * each
            yield from up_copies(up if k < ny else spare, 1, ny, at, outs[k], 0, sems, first)
            yield from down_copies(down, ny, side, at, outs[k], rows, sems, first + ups)

    @pl.when(core == 0)
    def _():
        for c in copies(gate, value):
            c.start()

    @pl.when(core == 1)
    def _():
        for c in copies(value, gate):
            c.start()

    for c in copies(gate, value):
        c.wait()


def packed_second(ny, gate, value, down):
    rows = gate.shape[1] * gate.shape[2] // ny // LANES + LAYERS * down.shape[1] // ny // 2
    each = gate.shape[2] // ny // LANES + LAYERS
    return pl.pallas_call(
        functools.partial(pack_second_kernel, ny),
        out_shape=[jax.ShapeDtypeStruct((rows, LANES), BF16)] * (ny + 1),
        in_specs=[HBM] * 3,
        out_specs=[VMEM] * (ny + 1),
        scratch_shapes=[pltpu.SemaphoreType.DMA(((ny + 1) * each,))],
        cost_estimate=cost(1000000, 2 * ny * rows * LANES),
        compiler_params=room(4),
        name="pack1",
    )(gate, value, down)


def high_and_low(squares):
    tokens = squares.shape[0]
    total = jnp.broadcast_to(jnp.sum(squares, axis=1, keepdims=True), (tokens, LANES)).T[0:EXTRA]
    high = total.astype(BF16).astype(F32)
    index = lax.broadcasted_iota(jnp.int32, (EXTRA, tokens), 0)
    return jnp.where(index == 0, high, jnp.where(index == 1, total - high, 0.0)).astype(BF16)


def multiplied(gained, weights, start, block, store):
    width = LANES
    wide = 2 * LANES
    for j in range(block // wide):
        weight = jnp.concatenate(
            [
                jnp.concatenate(
                    [w[pl.ds(start + (2 * j + i) * width, width), :] for i in range(2)], axis=1
                )
                for w in weights
            ],
            axis=0,
        )
        store(j * wide, jnp.dot(gained, weight, preferred_element_type=F32).T.astype(BF16))


def into_slots(out, rows, units):
    def store(first, result):
        low, end = first, first + result.shape[0]
        while low < end:
            slot = low // units
            high = min(end, (slot + 1) * units)
            out[slot, pl.ds(rows + (low - slot * units), high - low), :] = result[
                low - first : high - first
            ]
            low = high

    return store


def with_gain(values, gain_block, layer):
    return (values * gain_block.astype(F32)[8 * layer : 8 * layer + 1]).astype(BF16)


def first_up_kernel(side, start, ny, nz, block, *refs):
    mine = refs[0]
    out = refs[1] if side == 0 else refs[3]
    tokens = LANES
    units = block // nz
    core = lax.axis_index("dp")
    gained = jnp.concatenate(
        [
            with_gain(mine[k, 0:tokens, :].astype(F32), mine[k, tokens : tokens + 16, :], 0)
            for k in range(ny)
        ],
        axis=1,
    )
    if side == 0:
        weights = [mine.at[k] for k in range(ny)]
        multiplied(gained, weights, start, block, into_slots(out, 0, units))
        return
    other, near = refs[1], refs[2]
    weights = [other.at[k] for k in range(ny)]
    rows = pl.multiple_of((1 - core) * units, 16)
    multiplied(gained, weights, start, block, into_slots(out, rows, units))
    squares = jnp.zeros((tokens, LANES), F32)
    for k in range(ny):
        values = mine[k, 0:tokens, :].astype(F32)
        squares = squares + values * values
    both = high_and_low(squares)
    rows = pl.multiple_of(core * units, 16)
    refs[4][...] = mine[:, 0:start, :]
    for i in range(nz):
        out[i, pl.ds(rows, units), :] = near[i]
        out[i, 2 * units : 2 * units + EXTRA, :] = both


def first_projected(side, start, block, ny, nz, args):
    units = block // nz
    rows = units if side == 0 else 2 * units + EXTRA
    shapes = [jax.ShapeDtypeStruct((nz, rows, LANES), BF16)]
    if side:
        shapes.append(jax.ShapeDtypeStruct((ny, start, LANES), BF16))
    return pl.pallas_call(
        functools.partial(first_up_kernel, side, start, ny, nz, block),
        out_shape=shapes,
        in_specs=[VMEM] * len(args),
        out_specs=[VMEM] * len(shapes),
        cost_estimate=cost(2 * ny * LANES * LANES * block, 2 * ny * LANES * block),
        compiler_params=room(8),
    )(*args)


def second_up_kernel(ny, nz, block, *refs):
    mine, fresh = refs[:2]
    sides = [refs[2 : 2 + ny], refs[2 + ny : 2 + 2 * ny]]
    out, kept = refs[2 + 2 * ny :]
    tokens = LANES
    units = block // nz
    core = lax.axis_index("dp")
    y = lax.axis_index("y")
    squares = jnp.zeros((tokens, LANES), F32)
    gained = []
    for k in range(ny):
        at = lax.rem(y - k + ny, ny)
        values = fresh[:, at].astype(F32).reshape(tokens, LANES)
        if k == 0:
            kept[...] = values.astype(BF16)
        squares = squares + values * values
        gained.append(with_gain(values, mine[at, tokens : tokens + 16, :], 1))
    gained = jnp.concatenate(gained, axis=1)
    for side, weights in enumerate(sides):
        rows = pl.multiple_of((core if side == 0 else 1 - core) * units, 16)
        multiplied(gained, weights, 0, block, into_slots(out, rows, units))
    both = high_and_low(squares)
    for i in range(nz):
        out[i, 2 * units : 2 * units + EXTRA, :] = both


def second_projected(block, ny, nz, args):
    units = block // nz
    return pl.pallas_call(
        functools.partial(second_up_kernel, ny, nz, block),
        out_shape=[
            jax.ShapeDtypeStruct((nz, 2 * units + EXTRA, LANES), BF16),
            jax.ShapeDtypeStruct((LANES, LANES), BF16),
        ],
        in_specs=[VMEM] * len(args),
        out_specs=[VMEM] * 2,
        cost_estimate=cost(4 * ny * LANES * LANES * block, 4 * ny * LANES * block),
        compiler_params=room(8),
        name="up1",
    )(*args)


def mid_kernel(layer, length, parts, table, out):
    count, _, tokens = parts.shape
    units = out.shape[1]
    total = parts[0].astype(F32)
    for i in range(1, count):
        total = total + parts[i].astype(F32)
    mean = (total[2 * units : 2 * units + 1] + total[2 * units + 1 : 2 * units + 2]) / D
    scale = lax.rsqrt(mean + EPS)
    position = lax.rem(lax.broadcasted_iota(jnp.int32, (units, tokens), 1), length)
    spread = jnp.concatenate([table[layer]] * (LANES // 8), axis=0)
    columns = spread.T[0:units]

    def mixed(low, at):
        x = (total[low : low + units] * scale).astype(BF16).astype(F32)
        one = jnp.where(position >= 1, pltpu.roll(x, 1, 1), 0.0)
        two = jnp.where(position >= 2, pltpu.roll(x, 2, 1), 0.0)
        return (
            columns[:, at + 3 : at + 4]
            + two * columns[:, at : at + 1]
            + one * columns[:, at + 1 : at + 2]
            + x * columns[:, at + 2 : at + 3]
        )

    hidden = (jax.nn.gelu(mixed(0, 0)) * mixed(units, 4)).astype(BF16)
    for i in range(out.shape[0]):
        out[i] = hidden


def gated(layer, parts, table, units, length):
    return pl.pallas_call(
        functools.partial(mid_kernel, layer, length),
        out_shape=jax.ShapeDtypeStruct((parts.shape[0], units, parts.shape[2]), BF16),
        in_specs=[VMEM] * 2,
        out_specs=VMEM,
        cost_estimate=cost(1000000, parts.size * 2),
        compiler_params=room(6),
    )(parts, table)


def down_kernel(layer, start, half, ny, nx, hidden, *refs):
    out = refs[-1]
    sides = [refs[0:ny], refs[ny : 2 * ny]]
    nz, _, tokens = hidden.shape
    core = lax.axis_index("dp")
    y = lax.axis_index("y")
    term = 0.0
    for side, weights in enumerate(sides):
        first = (core if side == 0 else 1 - core) * (nz // 2)
        rows = hidden[pl.ds(first, nz // 2)].reshape(half, tokens).T
        weight = jnp.concatenate([w[pl.ds(start, half), :] for w in weights], axis=1)
        term = term + jnp.dot(rows, weight, preferred_element_type=F32)
    for k in range(ny):
        piece = term[:, k * LANES : (k + 1) * LANES]
        at = lax.rem(y - k + ny, ny)
        if layer == 0:
            out[:, at] = piece.reshape(ny * nx, -1, LANES).astype(BF16)
        else:
            for i in range(nx):
                out[at * nx + i] = piece.astype(BF16)


def lowered(layer, start, half, ny, nx, args):
    tokens = args[0].shape[2]
    count = ny * nx
    shape = (count, ny, tokens // count, LANES) if layer == 0 else (count, tokens, LANES)
    return pl.pallas_call(
        functools.partial(down_kernel, layer, start, half, ny, nx),
        out_shape=jax.ShapeDtypeStruct(shape, BF16),
        in_specs=[VMEM] * len(args),
        out_specs=VMEM,
        cost_estimate=cost(4 * half * ny * LANES * tokens, 4 * half * ny * LANES),
        compiler_params=room(8),
    )(*args)


def add_kernel(terms, mine, out):
    count, ny, piece, _ = terms.shape
    place = lax.axis_index("y") * (count // ny) + lax.axis_index("x")
    total = terms[0].astype(F32)
    for i in range(1, count):
        total = total + terms[i].astype(F32)
    rows = pl.multiple_of(place * piece, piece)
    own = mine[:, pl.ds(rows, piece), :].astype(F32)
    fresh = (0.5 * own + total).astype(BF16)
    for i in range(count):
        out[i] = fresh


def added(terms, mine):
    return pl.pallas_call(
        add_kernel,
        out_shape=jax.ShapeDtypeStruct(terms.shape, BF16),
        in_specs=[VMEM] * 2,
        out_specs=VMEM,
        cost_estimate=cost(1000000, terms.size * 4),
        compiler_params=room(4),
        name="add",
    )(terms, mine)


def last_kernel(terms, kept, last, out):
    total = terms[0].astype(F32)
    for i in range(1, terms.shape[0]):
        total = total + terms[i].astype(F32)
    fresh = (0.5 * kept[...].astype(F32) + total).astype(BF16)
    last[...] = fresh
    values = fresh.astype(F32)
    both = high_and_low(values * values)
    for i in range(out.shape[0]):
        out[i] = both


def finished(terms, kept, copies):
    return pl.pallas_call(
        last_kernel,
        out_shape=[
            jax.ShapeDtypeStruct(kept.shape, BF16),
            jax.ShapeDtypeStruct((copies, EXTRA, terms.shape[1]), BF16),
        ],
        in_specs=[VMEM] * 2,
        out_specs=[VMEM] * 2,
        cost_estimate=cost(1000000, terms.size * 4),
        compiler_params=room(4),
        name="last",
    )(terms, kept)


def norm_kernel(last, parts, gain, out):
    tokens = last.shape[0]
    total = parts[0].astype(F32)
    for i in range(1, parts.shape[0]):
        total = total + parts[i].astype(F32)
    scale = lax.rsqrt((total[0:1] + total[1:2]) / D + EPS)
    column = jnp.broadcast_to(scale, (LANES, tokens)).T
    values = last[...].astype(F32) * column * gain[...].astype(F32)
    out[...] = values.astype(BF16)


def normed(last, parts, gain):
    return pl.pallas_call(
        norm_kernel,
        out_shape=jax.ShapeDtypeStruct(last.shape, BF16),
        in_specs=[VMEM] * 3,
        out_specs=VMEM,
        cost_estimate=cost(1000000, last.size * 4),
        compiler_params=room(4),
        name="norm",
    )(last, parts, gain)


def layers(
    stream,
    norm_gain,
    gate_weight,
    value_weight,
    gate_taps,
    value_taps,
    gate_bias,
    value_bias,
    down_weight,
    final_gain,
):
    batch_rows, length, width = stream.shape
    tokens = batch_rows * length
    ny, nx, nz = lax.axis_size("y"), lax.axis_size("x"), lax.axis_size("z")
    block = gate_weight.shape[2] // ny
    half = block // 2
    units = block // nz
    start = tokens + LAYERS * 8
    swap = [(0, 1), (1, 0)]
    own = stream.reshape(tokens, width)

    mine = packed_first(ny, gate_weight, value_weight, own, norm_gain)
    mine = exchanged(mine, "y")
    other = lax.ppermute(mine, "dp", swap)
    (parts,) = first_projected(0, start, block, ny, nz, [mine])
    parts, state = first_projected(1, start, block, ny, nz, [mine, other, parts])
    parts = exchanged(parts, "z")

    later = packed_second(ny, gate_weight, value_weight, down_weight)
    lower = lax.axis_index("y") * block + lax.axis_index("z") * units
    table = jnp.concatenate(
        [gate_taps, gate_bias[:, None], value_taps, value_bias[:, None]], axis=1
    )
    table = lax.dynamic_slice_in_dim(table, lower, units, 2).astype(F32)
    table = jnp.pad(table, ((0, 0), (0, 0), (0, LANES - units)))
    *later, table = lax.optimization_barrier((*later, table))
    near = [later[0]]
    for k in range(1, ny):
        near.append(lax.ppermute(later[k], "y", [(i, (i + k) % ny) for i in range(ny)]))

    hidden = gated(0, parts, table, units, length)
    hidden = exchanged(hidden, "z")
    far = [later[ny]] + [lax.ppermute(piece, "dp", swap) for piece in near[1:]]
    terms = lowered(0, block, half, ny, nx, [hidden, *near, *far])
    terms = exchanged(terms, ("y", "x"))
    fresh = exchanged(added(terms, state), ("y", "x"))

    parts, kept = second_projected(block, ny, nz, [state, fresh, *near, *far])
    hidden = exchanged(gated(1, exchanged(parts, "z"), table, units, length), "z")
    terms = lowered(1, block + half, half, ny, nx, [hidden, *near, *far])
    terms = exchanged(terms, ("y", "x"))
    last, squares = finished(terms, kept, nz * ny)
    squares = exchanged(squares, ("z", "y"))
    mixed = normed(last, squares, final_gain[None])
    return mixed.reshape(batch_rows, length, width)


def solution(mesh):
    split = Mesh(
        mesh.devices.reshape(8, 4, mesh.shape["cb"], mesh.shape["dp"]), ("z", "y", "x", "dp")
    )
    ra = ("z", "y")
    return jax.shard_map(
        layers,
        mesh=split,
        in_specs=(
            P("dp", None, ra),
            P(None, ra),
            P(None, ra, "x"),
            P(None, ra, "x"),
            P(None, None, "x"),
            P(None, None, "x"),
            P(None, "x"),
            P(None, "x"),
            P(None, "x", ra),
            P(ra),
        ),
        out_specs=P("dp", None, ra),
        check_vma=False,
    )
```

```python
import functools

import jax
import jax.numpy as jnp
from jax import lax
from jax.experimental import pallas as pl
from jax.experimental.pallas import tpu as pltpu
from jax.sharding import Mesh
from jax.sharding import PartitionSpec as P


D = 4096
LAYERS = 2
LANES = 128
EXTRA = 8
WHOLE_VMEM = 67043328
EPS = 1e-06
F32 = jnp.float32
BF16 = jnp.bfloat16
VMEM = pl.BlockSpec(memory_space=pltpu.VMEM)
HBM = pl.BlockSpec(memory_space=pltpu.MemorySpace.HBM)


def exchanged(x, axis):
    return lax.all_to_all(x, axis, split_axis=0, concat_axis=0, tiled=True)


def room(mebibytes):
    return pltpu.CompilerParams(vmem_limit_bytes=mebibytes * 1024 * 1024)


def cost(flops, moved):
    return pl.CostEstimate(flops=flops, bytes_accessed=moved, transcendentals=0)


def up_copies(up, layer, ny, at, out, start, sems, first):
    width, columns = up.shape[1:]
    each = columns // ny // LANES
    for j in range(each):
        low = pl.multiple_of((at * each + j) * LANES, LANES)
        yield pltpu.make_async_copy(
            up.at[layer, :, pl.ds(low, LANES)],
            out.at[pl.ds(start + j * width, width), :],
            sems.at[first + j],
        )


def down_copies(down, ny, core, at, out, start, sems, first):
    half = down.shape[1] // ny // 2
    low = pl.multiple_of((at * 2 + core) * half, half)
    for layer in range(LAYERS):
        yield pltpu.make_async_copy(
            down.at[layer, pl.ds(low, half), :],
            out.at[pl.ds(start + layer * half, half), :],
            sems.at[first + layer],
        )


def pack_first_kernel(ny, gate, value, stream, gain, out, held, sems, more):
    tokens, width = stream.shape
    each = gate.shape[2] // ny // LANES
    start = tokens + LAYERS * 8
    core = lax.axis_index("dp")
    others = [
        pltpu.make_async_copy(stream, out.at[i, pl.ds(0, tokens), :], more.at[i]) for i in range(ny)
    ]
    others.append(pltpu.make_async_copy(gain, held, more.at[ny]))

    def copies(up):
        for i in range(ny):
            yield from up_copies(up, 0, ny, i, out.at[i], start, sems, i * each)

    @pl.when(core == 0)
    def _():
        for c in copies(gate):
            c.start()

    @pl.when(core == 1)
    def _():
        for c in copies(value):
            c.start()

    for c in others:
        c.start()
    others[-1].wait()
    gains = jnp.broadcast_to(held[...].astype(F32)[:, None, :], (LAYERS, 8, width))
    gains = gains.reshape(LAYERS * 8, width).astype(BF16)
    for i in range(ny):
        out[i, tokens : tokens + LAYERS * 8, :] = gains
    for c in others[:-1]:
        c.wait()
    for c in copies(gate):
        c.wait()


def packed_first(ny, gate, value, stream, gain):
    rows = gate.shape[1] * gate.shape[2] // ny // LANES
    rows += stream.shape[0] + LAYERS * 8
    each = gate.shape[2] // ny // LANES
    return pl.pallas_call(
        functools.partial(pack_first_kernel, ny),
        out_shape=jax.ShapeDtypeStruct((ny, rows, LANES), BF16),
        in_specs=[HBM] * 4,
        out_specs=VMEM,
        scratch_shapes=[
            pltpu.VMEM(gain.shape, BF16),
            pltpu.SemaphoreType.DMA((ny * each,)),
            pltpu.SemaphoreType.DMA((ny + 1,)),
        ],
        cost_estimate=cost(1000000, 2 * ny * rows * LANES),
        compiler_params=pltpu.CompilerParams(
            vmem_limit_bytes=WHOLE_VMEM - 2 * ny * rows * LANES - 16384
        ),
        name="pack0",
    )(gate, value, stream, gain)


def pack_second_kernel(ny, gate, value, down, *refs):
    outs, sems = refs[:-1], refs[-1]
    ups = gate.shape[2] // ny // LANES
    rows = ups * gate.shape[1]
    each = ups + LAYERS
    core = lax.axis_index("dp")
    y = lax.axis_index("y")

    def copies(up, spare):
        for k in range(ny + 1):
            at = lax.rem(y + k, ny) if k < ny else y
            side = core if k < ny else 1 - core
            first = k * each
            yield from up_copies(up if k < ny else spare, 1, ny, at, outs[k], 0, sems, first)
            yield from down_copies(down, ny, side, at, outs[k], rows, sems, first + ups)

    @pl.when(core == 0)
    def _():
        for c in copies(gate, value):
            c.start()

    @pl.when(core == 1)
    def _():
        for c in copies(value, gate):
            c.start()

    for c in copies(gate, value):
        c.wait()


def packed_second(ny, gate, value, down):
    rows = gate.shape[1] * gate.shape[2] // ny // LANES + LAYERS * down.shape[1] // ny // 2
    each = gate.shape[2] // ny // LANES + LAYERS
    return pl.pallas_call(
        functools.partial(pack_second_kernel, ny),
        out_shape=[jax.ShapeDtypeStruct((rows, LANES), BF16)] * (ny + 1),
        in_specs=[HBM] * 3,
        out_specs=[VMEM] * (ny + 1),
        scratch_shapes=[pltpu.SemaphoreType.DMA(((ny + 1) * each,))],
        cost_estimate=cost(1000000, 2 * ny * rows * LANES),
        compiler_params=room(4),
        name="pack1",
    )(gate, value, down)


def high_and_low(squares):
    tokens = squares.shape[0]
    total = jnp.broadcast_to(jnp.sum(squares, axis=1, keepdims=True), (tokens, LANES)).T[0:EXTRA]
    high = total.astype(BF16).astype(F32)
    index = lax.broadcasted_iota(jnp.int32, (EXTRA, tokens), 0)
    return jnp.where(index == 0, high, jnp.where(index == 1, total - high, 0.0)).astype(BF16)


def multiplied(gained, weights, start, block, store):
    width = LANES
    wide = 2 * LANES
    for j in range(block // wide):
        weight = jnp.concatenate(
            [
                jnp.concatenate(
                    [w[pl.ds(start + (2 * j + i) * width, width), :] for i in range(2)], axis=1
                )
                for w in weights
            ],
            axis=0,
        )
        store(j * wide, jnp.dot(gained, weight, preferred_element_type=F32).T.astype(BF16))


def into_slots(out, rows, units):
    def store(first, result):
        low, end = first, first + result.shape[0]
        while low < end:
            slot = low // units
            high = min(end, (slot + 1) * units)
            out[slot, pl.ds(rows + (low - slot * units), high - low), :] = result[
                low - first : high - first
            ]
            low = high

    return store


def with_gain(values, gain_block, layer):
    return (values * gain_block.astype(F32)[8 * layer : 8 * layer + 1]).astype(BF16)


def first_up_kernel(side, start, ny, nz, block, *refs):
    mine = refs[0]
    out = refs[1] if side == 0 else refs[3]
    tokens = LANES
    units = block // nz
    core = lax.axis_index("dp")
    gained = jnp.concatenate(
        [
            with_gain(mine[k, 0:tokens, :].astype(F32), mine[k, tokens : tokens + 16, :], 0)
            for k in range(ny)
        ],
        axis=1,
    )
    if side == 0:
        weights = [mine.at[k] for k in range(ny)]
        multiplied(gained, weights, start, block, into_slots(out, 0, units))
        return
    other, near = refs[1], refs[2]
    weights = [other.at[k] for k in range(ny)]
    rows = pl.multiple_of((1 - core) * units, 16)
    multiplied(gained, weights, start, block, into_slots(out, rows, units))
    squares = jnp.zeros((tokens, LANES), F32)
    for k in range(ny):
        values = mine[k, 0:tokens, :].astype(F32)
        squares = squares + values * values
    both = high_and_low(squares)
    rows = pl.multiple_of(core * units, 16)
    refs[4][...] = mine[:, 0:start, :]
    for i in range(nz):
        out[i, pl.ds(rows, units), :] = near[i]
        out[i, 2 * units : 2 * units + EXTRA, :] = both


def first_projected(side, start, block, ny, nz, args):
    units = block // nz
    rows = units if side == 0 else 2 * units + EXTRA
    shapes = [jax.ShapeDtypeStruct((nz, rows, LANES), BF16)]
    if side:
        shapes.append(jax.ShapeDtypeStruct((ny, start, LANES), BF16))
    return pl.pallas_call(
        functools.partial(first_up_kernel, side, start, ny, nz, block),
        out_shape=shapes,
        in_specs=[VMEM] * len(args),
        out_specs=[VMEM] * len(shapes),
        cost_estimate=cost(2 * ny * LANES * LANES * block, 2 * ny * LANES * block),
        compiler_params=room(8),
    )(*args)


def second_up_kernel(ny, nz, block, *refs):
    mine, fresh = refs[:2]
    sides = [refs[2 : 2 + ny], refs[2 + ny : 2 + 2 * ny]]
    out, kept = refs[2 + 2 * ny :]
    tokens = LANES
    units = block // nz
    core = lax.axis_index("dp")
    y = lax.axis_index("y")
    squares = jnp.zeros((tokens, LANES), F32)
    gained = []
    for k in range(ny):
        at = lax.rem(y - k + ny, ny)
        values = fresh[:, at].astype(F32).reshape(tokens, LANES)
        if k == 0:
            kept[...] = values.astype(BF16)
        squares = squares + values * values
        gained.append(with_gain(values, mine[at, tokens : tokens + 16, :], 1))
    gained = jnp.concatenate(gained, axis=1)
    for side, weights in enumerate(sides):
        rows = pl.multiple_of((core if side == 0 else 1 - core) * units, 16)
        multiplied(gained, weights, 0, block, into_slots(out, rows, units))
    both = high_and_low(squares)
    for i in range(nz):
        out[i, 2 * units : 2 * units + EXTRA, :] = both


def second_projected(block, ny, nz, args):
    units = block // nz
    return pl.pallas_call(
        functools.partial(second_up_kernel, ny, nz, block),
        out_shape=[
            jax.ShapeDtypeStruct((nz, 2 * units + EXTRA, LANES), BF16),
            jax.ShapeDtypeStruct((LANES, LANES), BF16),
        ],
        in_specs=[VMEM] * len(args),
        out_specs=[VMEM] * 2,
        cost_estimate=cost(4 * ny * LANES * LANES * block, 4 * ny * LANES * block),
        compiler_params=room(8),
        name="up1",
    )(*args)


def mid_kernel(layer, length, parts, table, out):
    count, _, tokens = parts.shape
    units = out.shape[1]
    total = parts[0].astype(F32)
    for i in range(1, count):
        total = total + parts[i].astype(F32)
    mean = (total[2 * units : 2 * units + 1] + total[2 * units + 1 : 2 * units + 2]) / D
    scale = lax.rsqrt(mean + EPS)
    position = lax.rem(lax.broadcasted_iota(jnp.int32, (units, tokens), 1), length)
    spread = jnp.concatenate([table[layer]] * (LANES // 8), axis=0)
    columns = spread.T[0:units]

    def mixed(low, at):
        x = (total[low : low + units] * scale).astype(BF16).astype(F32)
        one = jnp.where(position >= 1, pltpu.roll(x, 1, 1), 0.0)
        two = jnp.where(position >= 2, pltpu.roll(x, 2, 1), 0.0)
        return (
            columns[:, at + 3 : at + 4]
            + two * columns[:, at : at + 1]
            + one * columns[:, at + 1 : at + 2]
            + x * columns[:, at + 2 : at + 3]
        )

    hidden = (jax.nn.gelu(mixed(0, 0)) * mixed(units, 4)).astype(BF16)
    for i in range(out.shape[0]):
        out[i] = hidden


def gated(layer, parts, table, units, length):
    return pl.pallas_call(
        functools.partial(mid_kernel, layer, length),
        out_shape=jax.ShapeDtypeStruct((parts.shape[0], units, parts.shape[2]), BF16),
        in_specs=[VMEM] * 2,
        out_specs=VMEM,
        cost_estimate=cost(1000000, parts.size * 2),
        compiler_params=room(6),
    )(parts, table)


def down_kernel(layer, start, half, ny, nx, hidden, *refs):
    out = refs[-1]
    sides = [refs[0:ny], refs[ny : 2 * ny]]
    nz, _, tokens = hidden.shape
    core = lax.axis_index("dp")
    y = lax.axis_index("y")
    term = 0.0
    for side, weights in enumerate(sides):
        first = (core if side == 0 else 1 - core) * (nz // 2)
        rows = hidden[pl.ds(first, nz // 2)].reshape(half, tokens).T
        weight = jnp.concatenate([w[pl.ds(start, half), :] for w in weights], axis=1)
        term = term + jnp.dot(rows, weight, preferred_element_type=F32)
    for k in range(ny):
        piece = term[:, k * LANES : (k + 1) * LANES]
        at = lax.rem(y - k + ny, ny)
        if layer == 0:
            out[:, at] = piece.reshape(ny * nx, -1, LANES).astype(BF16)
        else:
            for i in range(nx):
                out[at * nx + i] = piece.astype(BF16)


def lowered(layer, start, half, ny, nx, args):
    tokens = args[0].shape[2]
    count = ny * nx
    shape = (count, ny, tokens // count, LANES) if layer == 0 else (count, tokens, LANES)
    return pl.pallas_call(
        functools.partial(down_kernel, layer, start, half, ny, nx),
        out_shape=jax.ShapeDtypeStruct(shape, BF16),
        in_specs=[VMEM] * len(args),
        out_specs=VMEM,
        cost_estimate=cost(4 * half * ny * LANES * tokens, 4 * half * ny * LANES),
        compiler_params=room(8),
    )(*args)


def half_kernel(start, half, ny, hidden, *refs):
    weights, out = refs[:ny], refs[ny]
    nz, _, tokens = hidden.shape
    core = lax.axis_index("dp")
    rows = hidden[pl.ds(core * (nz // 2), nz // 2)].reshape(half, tokens).T
    weight = jnp.concatenate([w[pl.ds(start, half), :] for w in weights], axis=1)
    out[...] = jnp.dot(rows, weight, preferred_element_type=F32)


def half_lowered(start, half, ny, args):
    tokens = args[0].shape[2]
    return pl.pallas_call(
        functools.partial(half_kernel, start, half, ny),
        out_shape=jax.ShapeDtypeStruct((tokens, ny * LANES), F32),
        in_specs=[VMEM] * len(args),
        out_specs=VMEM,
        cost_estimate=cost(2 * half * ny * LANES * tokens, 2 * half * ny * LANES),
        compiler_params=room(8),
        name="down00",
    )(*args)


def rest_kernel(start, half, ny, nx, hidden, term, *refs):
    weights, out = refs[:ny], refs[ny]
    nz, _, tokens = hidden.shape
    core = lax.axis_index("dp")
    y = lax.axis_index("y")
    rows = hidden[pl.ds((1 - core) * (nz // 2), nz // 2)].reshape(half, tokens).T
    weight = jnp.concatenate([w[pl.ds(start, half), :] for w in weights], axis=1)
    total = term[...] + jnp.dot(rows, weight, preferred_element_type=F32)
    for k in range(ny):
        piece = total[:, k * LANES : (k + 1) * LANES]
        out[:, lax.rem(y - k + ny, ny)] = piece.reshape(ny * nx, -1, LANES).astype(BF16)


def rest_lowered(start, half, ny, nx, args):
    tokens = args[0].shape[2]
    count = ny * nx
    return pl.pallas_call(
        functools.partial(rest_kernel, start, half, ny, nx),
        out_shape=jax.ShapeDtypeStruct((count, ny, tokens // count, LANES), BF16),
        in_specs=[VMEM] * len(args),
        out_specs=VMEM,
        cost_estimate=cost(2 * half * ny * LANES * tokens, 2 * half * ny * LANES),
        compiler_params=room(8),
        name="down01",
    )(*args)


def add_kernel(terms, mine, out):
    count, ny, piece, _ = terms.shape
    place = lax.axis_index("y") * (count // ny) + lax.axis_index("x")
    total = terms[0].astype(F32)
    for i in range(1, count):
        total = total + terms[i].astype(F32)
    rows = pl.multiple_of(place * piece, piece)
    own = mine[:, pl.ds(rows, piece), :].astype(F32)
    fresh = (0.5 * own + total).astype(BF16)
    for i in range(count):
        out[i] = fresh


def added(terms, mine):
    return pl.pallas_call(
        add_kernel,
        out_shape=jax.ShapeDtypeStruct(terms.shape, BF16),
        in_specs=[VMEM] * 2,
        out_specs=VMEM,
        cost_estimate=cost(1000000, terms.size * 4),
        compiler_params=room(4),
        name="add",
    )(terms, mine)


def last_kernel(terms, kept, last, out):
    total = terms[0].astype(F32)
    for i in range(1, terms.shape[0]):
        total = total + terms[i].astype(F32)
    fresh = (0.5 * kept[...].astype(F32) + total).astype(BF16)
    last[...] = fresh
    values = fresh.astype(F32)
    both = high_and_low(values * values)
    for i in range(out.shape[0]):
        out[i] = both


def finished(terms, kept, copies):
    return pl.pallas_call(
        last_kernel,
        out_shape=[
            jax.ShapeDtypeStruct(kept.shape, BF16),
            jax.ShapeDtypeStruct((copies, EXTRA, terms.shape[1]), BF16),
        ],
        in_specs=[VMEM] * 2,
        out_specs=[VMEM] * 2,
        cost_estimate=cost(1000000, terms.size * 4),
        compiler_params=room(4),
        name="last",
    )(terms, kept)


def norm_kernel(last, parts, gain, out):
    tokens = last.shape[0]
    total = parts[0].astype(F32)
    for i in range(1, parts.shape[0]):
        total = total + parts[i].astype(F32)
    scale = lax.rsqrt((total[0:1] + total[1:2]) / D + EPS)
    column = jnp.broadcast_to(scale, (LANES, tokens)).T
    values = last[...].astype(F32) * column * gain[...].astype(F32)
    out[...] = values.astype(BF16)


def normed(last, parts, gain):
    return pl.pallas_call(
        norm_kernel,
        out_shape=jax.ShapeDtypeStruct(last.shape, BF16),
        in_specs=[VMEM] * 3,
        out_specs=VMEM,
        cost_estimate=cost(1000000, last.size * 4),
        compiler_params=room(4),
        name="norm",
    )(last, parts, gain)


def layers(
    stream,
    norm_gain,
    gate_weight,
    value_weight,
    gate_taps,
    value_taps,
    gate_bias,
    value_bias,
    down_weight,
    final_gain,
):
    batch_rows, length, width = stream.shape
    tokens = batch_rows * length
    ny, nx, nz = lax.axis_size("y"), lax.axis_size("x"), lax.axis_size("z")
    block = gate_weight.shape[2] // ny
    half = block // 2
    units = block // nz
    start = tokens + LAYERS * 8
    swap = [(0, 1), (1, 0)]
    own = stream.reshape(tokens, width)

    mine = packed_first(ny, gate_weight, value_weight, own, norm_gain)
    mine = exchanged(mine, "y")
    other = lax.ppermute(mine, "dp", swap)
    (parts,) = first_projected(0, start, block, ny, nz, [mine])
    parts, state = first_projected(1, start, block, ny, nz, [mine, other, parts])
    parts = exchanged(parts, "z")

    later = packed_second(ny, gate_weight, value_weight, down_weight)
    lower = lax.axis_index("y") * block + lax.axis_index("z") * units
    table = jnp.concatenate(
        [gate_taps, gate_bias[:, None], value_taps, value_bias[:, None]], axis=1
    )
    table = lax.dynamic_slice_in_dim(table, lower, units, 2).astype(F32)
    table = jnp.pad(table, ((0, 0), (0, 0), (0, LANES - units)))
    *later, table = lax.optimization_barrier((*later, table))
    near = [later[0]]
    for k in range(1, ny):
        near.append(lax.ppermute(later[k], "y", [(i, (i + k) % ny) for i in range(ny)]))

    hidden = gated(0, parts, table, units, length)
    hidden = exchanged(hidden, "z")
    far = [later[ny]] + [lax.ppermute(piece, "dp", swap) for piece in near[1:]]
    terms = half_lowered(block, half, ny, [hidden, *near])
    terms = rest_lowered(block, half, ny, nx, [hidden, terms, *far])
    terms = exchanged(terms, ("y", "x"))
    fresh = exchanged(added(terms, state), ("y", "x"))

    parts, kept = second_projected(block, ny, nz, [state, fresh, *near, *far])
    hidden = exchanged(gated(1, exchanged(parts, "z"), table, units, length), "z")
    terms = lowered(1, block + half, half, ny, nx, [hidden, *near, *far])
    terms = exchanged(terms, ("y", "x"))
    last, squares = finished(terms, kept, nz * ny)
    squares = exchanged(squares, ("z", "y"))
    mixed = normed(last, squares, final_gain[None])
    return mixed.reshape(batch_rows, length, width)


def solution(mesh):
    split = Mesh(
        mesh.devices.reshape(8, 4, mesh.shape["cb"], mesh.shape["dp"]), ("z", "y", "x", "dp")
    )
    ra = ("z", "y")
    return jax.shard_map(
        layers,
        mesh=split,
        in_specs=(
            P("dp", None, ra),
            P(None, ra),
            P(None, ra, "x"),
            P(None, ra, "x"),
            P(None, None, "x"),
            P(None, None, "x"),
            P(None, "x"),
            P(None, "x"),
            P(None, "x", ra),
            P(ra),
        ),
        out_specs=P("dp", None, ra),
        check_vma=False,
    )
```

```python
import functools

import jax
import jax.numpy as jnp
from jax import lax
from jax.experimental import pallas as pl
from jax.experimental.pallas import tpu as pltpu
from jax.sharding import Mesh
from jax.sharding import PartitionSpec as P


D = 4096
LAYERS = 2
LANES = 128
EXTRA = 8
WHOLE_VMEM = 67043328
EPS = 1e-06
F32 = jnp.float32
BF16 = jnp.bfloat16
VMEM = pl.BlockSpec(memory_space=pltpu.VMEM)
HBM = pl.BlockSpec(memory_space=pltpu.MemorySpace.HBM)


def exchanged(x, axis):
    return lax.all_to_all(x, axis, split_axis=0, concat_axis=0, tiled=True)


def room(mebibytes):
    return pltpu.CompilerParams(vmem_limit_bytes=mebibytes * 1024 * 1024)


def cost(flops, moved):
    return pl.CostEstimate(flops=flops, bytes_accessed=moved, transcendentals=0)


def up_copies(up, layer, ny, at, out, start, sems, first):
    width, columns = up.shape[1:]
    each = columns // ny // LANES
    for j in range(each):
        low = pl.multiple_of((at * each + j) * LANES, LANES)
        yield pltpu.make_async_copy(
            up.at[layer, :, pl.ds(low, LANES)],
            out.at[pl.ds(start + j * width, width), :],
            sems.at[first + j],
        )


def down_copies(down, ny, core, at, out, start, sems, first):
    half = down.shape[1] // ny // 2
    low = pl.multiple_of((at * 2 + core) * half, half)
    for layer in range(LAYERS):
        yield pltpu.make_async_copy(
            down.at[layer, pl.ds(low, half), :],
            out.at[pl.ds(start + layer * half, half), :],
            sems.at[first + layer],
        )


def pack_first_kernel(ny, gate, value, stream, gain, out, held, sems, more):
    tokens, width = stream.shape
    each = gate.shape[2] // ny // LANES
    start = tokens + LAYERS * 8
    core = lax.axis_index("dp")
    others = [
        pltpu.make_async_copy(stream, out.at[i, pl.ds(0, tokens), :], more.at[i]) for i in range(ny)
    ]
    others.append(pltpu.make_async_copy(gain, held, more.at[ny]))

    def copies(up):
        for i in range(ny):
            yield from up_copies(up, 0, ny, i, out.at[i], start, sems, i * each)

    @pl.when(core == 0)
    def _():
        for c in copies(gate):
            c.start()

    @pl.when(core == 1)
    def _():
        for c in copies(value):
            c.start()

    for c in others:
        c.start()
    others[-1].wait()
    gains = jnp.broadcast_to(held[...].astype(F32)[:, None, :], (LAYERS, 8, width))
    gains = gains.reshape(LAYERS * 8, width).astype(BF16)
    for i in range(ny):
        out[i, tokens : tokens + LAYERS * 8, :] = gains
    for c in others[:-1]:
        c.wait()
    for c in copies(gate):
        c.wait()


def packed_first(ny, gate, value, stream, gain):
    rows = gate.shape[1] * gate.shape[2] // ny // LANES
    rows += stream.shape[0] + LAYERS * 8
    each = gate.shape[2] // ny // LANES
    return pl.pallas_call(
        functools.partial(pack_first_kernel, ny),
        out_shape=jax.ShapeDtypeStruct((ny, rows, LANES), BF16),
        in_specs=[HBM] * 4,
        out_specs=VMEM,
        scratch_shapes=[
            pltpu.VMEM(gain.shape, BF16),
            pltpu.SemaphoreType.DMA((ny * each,)),
            pltpu.SemaphoreType.DMA((ny + 1,)),
        ],
        cost_estimate=cost(1000000, 2 * ny * rows * LANES),
        compiler_params=pltpu.CompilerParams(
            vmem_limit_bytes=WHOLE_VMEM - 2 * ny * rows * LANES - 16384
        ),
        name="pack0",
    )(gate, value, stream, gain)


def pack_second_kernel(ny, gate, value, down, *refs):
    outs, sems = refs[:-1], refs[-1]
    ups = gate.shape[2] // ny // LANES
    rows = ups * gate.shape[1]
    each = ups + LAYERS
    core = lax.axis_index("dp")
    y = lax.axis_index("y")

    def copies(up, spare):
        for k in range(ny + 1):
            at = lax.rem(y + k, ny) if k < ny else y
            side = core if k < ny else 1 - core
            first = k * each
            yield from up_copies(up if k < ny else spare, 1, ny, at, outs[k], 0, sems, first)
            yield from down_copies(down, ny, side, at, outs[k], rows, sems, first + ups)

    @pl.when(core == 0)
    def _():
        for c in copies(gate, value):
            c.start()

    @pl.when(core == 1)
    def _():
        for c in copies(value, gate):
            c.start()

    for c in copies(gate, value):
        c.wait()


def packed_second(ny, gate, value, down):
    rows = gate.shape[1] * gate.shape[2] // ny // LANES + LAYERS * down.shape[1] // ny // 2
    each = gate.shape[2] // ny // LANES + LAYERS
    return pl.pallas_call(
        functools.partial(pack_second_kernel, ny),
        out_shape=[jax.ShapeDtypeStruct((rows, LANES), BF16)] * (ny + 1),
        in_specs=[HBM] * 3,
        out_specs=[VMEM] * (ny + 1),
        scratch_shapes=[pltpu.SemaphoreType.DMA(((ny + 1) * each,))],
        cost_estimate=cost(1000000, 2 * ny * rows * LANES),
        compiler_params=room(4),
        name="pack1",
    )(gate, value, down)


def high_and_low(squares):
    tokens = squares.shape[0]
    total = jnp.broadcast_to(jnp.sum(squares, axis=1, keepdims=True), (tokens, LANES)).T[0:EXTRA]
    high = total.astype(BF16).astype(F32)
    index = lax.broadcasted_iota(jnp.int32, (EXTRA, tokens), 0)
    return jnp.where(index == 0, high, jnp.where(index == 1, total - high, 0.0)).astype(BF16)


def multiplied(gained, weights, start, block, store):
    width = LANES
    wide = 2 * LANES
    for j in range(block // wide):
        weight = jnp.concatenate(
            [
                jnp.concatenate(
                    [w[pl.ds(start + (2 * j + i) * width, width), :] for i in range(2)], axis=1
                )
                for w in weights
            ],
            axis=0,
        )
        store(j * wide, jnp.dot(gained, weight, preferred_element_type=F32).T.astype(BF16))


def into_slots(out, rows, units):
    def store(first, result):
        low, end = first, first + result.shape[0]
        while low < end:
            slot = low // units
            high = min(end, (slot + 1) * units)
            out[slot, pl.ds(rows + (low - slot * units), high - low), :] = result[
                low - first : high - first
            ]
            low = high

    return store


def with_gain(values, gain_block, layer):
    return (values * gain_block.astype(F32)[8 * layer : 8 * layer + 1]).astype(BF16)


def first_up_kernel(side, start, ny, nz, block, *refs):
    mine = refs[0]
    out = refs[1] if side == 0 else refs[3]
    tokens = LANES
    units = block // nz
    core = lax.axis_index("dp")
    gained = jnp.concatenate(
        [
            with_gain(mine[k, 0:tokens, :].astype(F32), mine[k, tokens : tokens + 16, :], 0)
            for k in range(ny)
        ],
        axis=1,
    )
    if side == 0:
        weights = [mine.at[k] for k in range(ny)]
        multiplied(gained, weights, start, block, into_slots(out, 0, units))
        return
    other, near = refs[1], refs[2]
    weights = [other.at[k] for k in range(ny)]
    rows = pl.multiple_of((1 - core) * units, 16)
    multiplied(gained, weights, start, block, into_slots(out, rows, units))
    squares = jnp.zeros((tokens, LANES), F32)
    for k in range(ny):
        values = mine[k, 0:tokens, :].astype(F32)
        squares = squares + values * values
    both = high_and_low(squares)
    rows = pl.multiple_of(core * units, 16)
    refs[4][...] = mine[:, 0:start, :]
    for i in range(nz):
        out[i, pl.ds(rows, units), :] = near[i]
        out[i, 2 * units : 2 * units + EXTRA, :] = both


def first_projected(side, start, block, ny, nz, args):
    units = block // nz
    rows = units if side == 0 else 2 * units + EXTRA
    shapes = [jax.ShapeDtypeStruct((nz, rows, LANES), BF16)]
    if side:
        shapes.append(jax.ShapeDtypeStruct((ny, start, LANES), BF16))
    return pl.pallas_call(
        functools.partial(first_up_kernel, side, start, ny, nz, block),
        out_shape=shapes,
        in_specs=[VMEM] * len(args),
        out_specs=[VMEM] * len(shapes),
        cost_estimate=cost(2 * ny * LANES * LANES * block, 2 * ny * LANES * block),
        compiler_params=room(8),
    )(*args)


def second_up_kernel(ny, nz, block, *refs):
    mine, fresh = refs[:2]
    sides = [refs[2 : 2 + ny], refs[2 + ny : 2 + 2 * ny]]
    out, kept = refs[2 + 2 * ny :]
    tokens = LANES
    units = block // nz
    core = lax.axis_index("dp")
    y = lax.axis_index("y")
    squares = jnp.zeros((tokens, LANES), F32)
    gained = []
    for k in range(ny):
        at = lax.rem(y - k + ny, ny)
        values = fresh[:, at].astype(F32).reshape(tokens, LANES)
        if k == 0:
            kept[...] = values.astype(BF16)
        squares = squares + values * values
        gained.append(with_gain(values, mine[at, tokens : tokens + 16, :], 1))
    gained = jnp.concatenate(gained, axis=1)
    for side, weights in enumerate(sides):
        rows = pl.multiple_of((core if side == 0 else 1 - core) * units, 16)
        multiplied(gained, weights, 0, block, into_slots(out, rows, units))
    both = high_and_low(squares)
    for i in range(nz):
        out[i, 2 * units : 2 * units + EXTRA, :] = both


def second_projected(block, ny, nz, args):
    units = block // nz
    return pl.pallas_call(
        functools.partial(second_up_kernel, ny, nz, block),
        out_shape=[
            jax.ShapeDtypeStruct((nz, 2 * units + EXTRA, LANES), BF16),
            jax.ShapeDtypeStruct((LANES, LANES), BF16),
        ],
        in_specs=[VMEM] * len(args),
        out_specs=[VMEM] * 2,
        cost_estimate=cost(4 * ny * LANES * LANES * block, 4 * ny * LANES * block),
        compiler_params=room(8),
        name="up1",
    )(*args)


def mid_kernel(layer, length, parts, table, out):
    count, _, tokens = parts.shape
    units = out.shape[1]
    total = parts[0].astype(F32)
    for i in range(1, count):
        total = total + parts[i].astype(F32)
    mean = (total[2 * units : 2 * units + 1] + total[2 * units + 1 : 2 * units + 2]) / D
    scale = lax.rsqrt(mean + EPS)
    position = lax.rem(lax.broadcasted_iota(jnp.int32, (units, tokens), 1), length)
    spread = jnp.concatenate([table[layer]] * (LANES // 8), axis=0)
    columns = spread.T[0:units]

    def mixed(low, at):
        x = (total[low : low + units] * scale).astype(BF16).astype(F32)
        one = jnp.where(position >= 1, pltpu.roll(x, 1, 1), 0.0)
        two = jnp.where(position >= 2, pltpu.roll(x, 2, 1), 0.0)
        return (
            columns[:, at + 3 : at + 4]
            + two * columns[:, at : at + 1]
            + one * columns[:, at + 1 : at + 2]
            + x * columns[:, at + 2 : at + 3]
        )

    hidden = (jax.nn.gelu(mixed(0, 0)) * mixed(units, 4)).astype(BF16)
    for i in range(out.shape[0]):
        out[i] = hidden


def gated(layer, parts, table, units, length):
    return pl.pallas_call(
        functools.partial(mid_kernel, layer, length),
        out_shape=jax.ShapeDtypeStruct((parts.shape[0], units, parts.shape[2]), BF16),
        in_specs=[VMEM] * 2,
        out_specs=VMEM,
        cost_estimate=cost(1000000, parts.size * 2),
        compiler_params=room(6),
    )(parts, table)


def down_kernel(layer, start, half, ny, nx, hidden, *refs):
    out = refs[-1]
    sides = [refs[0:ny], refs[ny : 2 * ny]]
    nz, _, tokens = hidden.shape
    core = lax.axis_index("dp")
    y = lax.axis_index("y")
    term = 0.0
    for side, weights in enumerate(sides):
        first = (core if side == 0 else 1 - core) * (nz // 2)
        rows = hidden[pl.ds(first, nz // 2)].reshape(half, tokens).T
        weight = jnp.concatenate([w[pl.ds(start, half), :] for w in weights], axis=1)
        term = term + jnp.dot(rows, weight, preferred_element_type=F32)
    for k in range(ny):
        piece = term[:, k * LANES : (k + 1) * LANES]
        at = lax.rem(y - k + ny, ny)
        if layer == 0:
            out[:, at] = piece.reshape(ny * nx, -1, LANES).astype(BF16)
        else:
            for i in range(nx):
                out[i * ny + at] = piece.astype(BF16)


def lowered(layer, start, half, ny, nx, args):
    tokens = args[0].shape[2]
    count = ny * nx
    shape = (count, ny, tokens // count, LANES) if layer == 0 else (count, tokens, LANES)
    return pl.pallas_call(
        functools.partial(down_kernel, layer, start, half, ny, nx),
        out_shape=jax.ShapeDtypeStruct(shape, BF16),
        in_specs=[VMEM] * len(args),
        out_specs=VMEM,
        cost_estimate=cost(4 * half * ny * LANES * tokens, 4 * half * ny * LANES),
        compiler_params=room(8),
    )(*args)


def add_kernel(terms, mine, out):
    count, ny, piece, _ = terms.shape
    place = lax.axis_index("x") * ny + lax.axis_index("y")
    total = terms[0].astype(F32)
    for i in range(1, count):
        total = total + terms[i].astype(F32)
    rows = pl.multiple_of(place * piece, piece)
    own = mine[:, pl.ds(rows, piece), :].astype(F32)
    fresh = (0.5 * own + total).astype(BF16)
    for i in range(count):
        out[i] = fresh


def added(terms, mine):
    return pl.pallas_call(
        add_kernel,
        out_shape=jax.ShapeDtypeStruct(terms.shape, BF16),
        in_specs=[VMEM] * 2,
        out_specs=VMEM,
        cost_estimate=cost(1000000, terms.size * 4),
        compiler_params=room(4),
        name="add",
    )(terms, mine)


def last_kernel(terms, kept, last, out):
    total = terms[0].astype(F32)
    for i in range(1, terms.shape[0]):
        total = total + terms[i].astype(F32)
    fresh = (0.5 * kept[...].astype(F32) + total).astype(BF16)
    last[...] = fresh
    values = fresh.astype(F32)
    both = high_and_low(values * values)
    for i in range(out.shape[0]):
        out[i] = both


def finished(terms, kept, copies):
    return pl.pallas_call(
        last_kernel,
        out_shape=[
            jax.ShapeDtypeStruct(kept.shape, BF16),
            jax.ShapeDtypeStruct((copies, EXTRA, terms.shape[1]), BF16),
        ],
        in_specs=[VMEM] * 2,
        out_specs=[VMEM] * 2,
        cost_estimate=cost(1000000, terms.size * 4),
        compiler_params=room(4),
        name="last",
    )(terms, kept)


def norm_kernel(last, parts, gain, out):
    tokens = last.shape[0]
    total = parts[0].astype(F32)
    for i in range(1, parts.shape[0]):
        total = total + parts[i].astype(F32)
    scale = lax.rsqrt((total[0:1] + total[1:2]) / D + EPS)
    column = jnp.broadcast_to(scale, (LANES, tokens)).T
    values = last[...].astype(F32) * column * gain[...].astype(F32)
    out[...] = values.astype(BF16)


def normed(last, parts, gain):
    return pl.pallas_call(
        norm_kernel,
        out_shape=jax.ShapeDtypeStruct(last.shape, BF16),
        in_specs=[VMEM] * 3,
        out_specs=VMEM,
        cost_estimate=cost(1000000, last.size * 4),
        compiler_params=room(4),
        name="norm",
    )(last, parts, gain)


def layers(
    stream,
    norm_gain,
    gate_weight,
    value_weight,
    gate_taps,
    value_taps,
    gate_bias,
    value_bias,
    down_weight,
    final_gain,
):
    batch_rows, length, width = stream.shape
    tokens = batch_rows * length
    ny, nx, nz = lax.axis_size("y"), lax.axis_size("x"), lax.axis_size("z")
    block = gate_weight.shape[2] // ny
    half = block // 2
    units = block // nz
    start = tokens + LAYERS * 8
    swap = [(0, 1), (1, 0)]
    own = stream.reshape(tokens, width)

    mine = packed_first(ny, gate_weight, value_weight, own, norm_gain)
    mine = exchanged(mine, "y")
    other = lax.ppermute(mine, "dp", swap)
    (parts,) = first_projected(0, start, block, ny, nz, [mine])
    parts, state = first_projected(1, start, block, ny, nz, [mine, other, parts])
    parts = exchanged(parts, "z")

    later = packed_second(ny, gate_weight, value_weight, down_weight)
    lower = lax.axis_index("y") * block + lax.axis_index("z") * units
    table = jnp.concatenate(
        [gate_taps, gate_bias[:, None], value_taps, value_bias[:, None]], axis=1
    )
    table = lax.dynamic_slice_in_dim(table, lower, units, 2).astype(F32)
    table = jnp.pad(table, ((0, 0), (0, 0), (0, LANES - units)))
    *later, table = lax.optimization_barrier((*later, table))
    near = [later[0]]
    for k in range(1, ny):
        near.append(lax.ppermute(later[k], "y", [(i, (i + k) % ny) for i in range(ny)]))

    hidden = gated(0, parts, table, units, length)
    hidden = exchanged(hidden, "z")
    far = [later[ny]] + [lax.ppermute(piece, "dp", swap) for piece in near[1:]]
    terms = lowered(0, block, half, ny, nx, [hidden, *near, *far])
    terms = exchanged(terms, ("x", "y"))
    fresh = exchanged(added(terms, state), ("x", "y"))

    parts, kept = second_projected(block, ny, nz, [state, fresh, *near, *far])
    hidden = exchanged(gated(1, exchanged(parts, "z"), table, units, length), "z")
    terms = lowered(1, block + half, half, ny, nx, [hidden, *near, *far])
    terms = exchanged(terms, ("x", "y"))
    last, squares = finished(terms, kept, nz * ny)
    squares = exchanged(squares, ("y", "z"))
    mixed = normed(last, squares, final_gain[None])
    return mixed.reshape(batch_rows, length, width)


def solution(mesh):
    split = Mesh(
        mesh.devices.reshape(8, 4, mesh.shape["cb"], mesh.shape["dp"]), ("z", "y", "x", "dp")
    )
    ra = ("z", "y")
    return jax.shard_map(
        layers,
        mesh=split,
        in_specs=(
            P("dp", None, ra),
            P(None, ra),
            P(None, ra, "x"),
            P(None, ra, "x"),
            P(None, None, "x"),
            P(None, None, "x"),
            P(None, "x"),
            P(None, "x"),
            P(None, "x", ra),
            P(ra),
        ),
        out_specs=P("dp", None, ra),
        check_vma=False,
    )
```
